32 devices in a mesh: fs: 8 (over z, core), tp: 4 (over y, x).
Axes of the slice: x: 2, y: 2, z: 4, core: 2. Of those that a mesh axis runs over, the one named last changes fastest.
Arguments:
- tokens: bfloat16 [4096, 2048], P('fs'), may hold values from -6 to 6
- cotangent: bfloat16 [4096, 2048], P('fs'), may hold values from -6 to 6
- gate_weight: bfloat16 [2048, 2816], P('fs', 'tp'), may hold values from -0.125 to 0.125
- up_weight: bfloat16 [2048, 2816], P('fs', 'tp'), may hold values from -0.125 to 0.125
- down_weight: bfloat16 [2048, 2816], P('fs', 'tp'), may hold values from -0.109375 to 0.109375
Outputs:
- input_grad: bfloat16 [4096, 2048], P('fs', 'tp')
- gate_grad: float32 [2048, 2816], P('fs', 'tp')
- up_grad: float32 [2048, 2816], P('fs', 'tp')
- down_grad: float32 [2048, 2816], P('fs', 'tp')
The draws below stay inside these ranges and needn't reach their ends.
All inputs are finite; a program needn't handle non-finite values.
Results may differ from the reference program's by a relative error of at most 0.014.
Values may be sent and summed in bfloat16 or wider, within the bound.
A program may use at most 64 MiB of HBM per device.

```python
import jax
import jax.numpy as jnp
from jax import lax

D = 2048
FF = 2816
TOKENS = 4096
N_TP = 4


def with_spikes(array, own_key, source, target, shards_of, factor):
    owner, partner = [(jnp.arange(array.shape[position]) // (array.shape[position] // shards_of)).reshape([-1 if axis == position else 1 for axis in range(array.ndim)]) for position in (source, target)]
    chosen = jax.random.permutation(own_key, shards_of)[partner]
    strong = (owner == chosen) | (owner == (partner + shards_of // 2) % shards_of)
    return jnp.where(strong, factor * array, array)


def block_levels(stream_key, dims, split, smallest, high):
    def one(position, shards_of):
        draws = jax.random.uniform(jax.random.fold_in(jax.random.fold_in(stream_key, 6), position), (shards_of,), jnp.float32, smallest / len(split), high / len(split))
        return jnp.repeat(jnp.exp(draws), dims[position] // shards_of).reshape((-1,) + (1,) * (len(dims) - position - 1))

    gain = one(*split[0])
    for cut in split[1:]:
        gain = gain * one(*cut)
    return gain


def centred(stream_key, extent, scale, limit, pieces=(), kind=jnp.bfloat16):
    values = jax.random.normal(stream_key, extent, jnp.float32) * scale
    if len(pieces) > 0:
        values = block_levels(stream_key, extent, pieces, -0.22, 0.18) * values
    return jnp.clip(values, min=-limit, max=limit).astype(kind)


def heavy_noise(stream_key, dims, scale, most, pieces, heavy, kind=jnp.bfloat16):
    drawn = scale * jax.random.normal(stream_key, dims, jnp.float32)
    if pieces:
        drawn = drawn * block_levels(stream_key, dims, pieces, -0.22, 0.18)
    return jnp.clip(with_spikes(drawn, jax.random.fold_in(stream_key, 3), *heavy), -most, most).astype(kind)


def setup_inputs(seed: int = 0) -> dict:
    streams_of = jax.random.split(jax.random.key(seed), 6)
    tokens = centred(streams_of[0], (TOKENS, D), 1.0, 6.0, ((0, 8),))
    cotangent = heavy_noise(streams_of[1], (TOKENS, D), 1.0, 6.0, ((0, 8),), (0, 1, 8, 2.0))
    gate_weight = centred(streams_of[2], (D, FF), D ** -0.5, 0.125, ((0, 8), (1, 4)))
    up_weight = centred(streams_of[3], (D, FF), D ** -0.5, 0.125, ((0, 8), (1, 4)))
    down_weight = centred(streams_of[4], (D, FF), FF ** -0.5, 0.109375, ((0, 8), (1, 4)))
    return dict(tokens=tokens, cotangent=cotangent, gate_weight=gate_weight, up_weight=up_weight, down_weight=down_weight)


def reference(tokens, cotangent, gate_weight, up_weight, down_weight):
    gate = jnp.dot(tokens, gate_weight, preferred_element_type=jnp.float32)
    up = jnp.dot(tokens, up_weight, preferred_element_type=jnp.float32)
    sig = jax.nn.sigmoid(gate)
    act = gate * sig
    hidden = (act * up).astype(jnp.bfloat16)
    hidden_grad = lax.dot_general(cotangent, down_weight, (((1,), (0,)), ((), ())), preferred_element_type=jnp.float32)
    gate_cot = (hidden_grad * up * sig * (1.0 + gate * (1.0 - sig))).astype(jnp.bfloat16)
    up_cot = (hidden_grad * act).astype(jnp.bfloat16)
    width = FF // N_TP

    def add_block(total, index):
        start = (index * width).astype(jnp.int32)
        gate_part = lax.dynamic_slice_in_dim(gate_cot, start, width, 1)
        up_part = lax.dynamic_slice_in_dim(up_cot, start, width, 1)
        gate_rows = lax.dynamic_slice_in_dim(gate_weight, start, width, 1)
        up_rows = lax.dynamic_slice_in_dim(up_weight, start, width, 1)
        partial_value = lax.dot_general(gate_part, gate_rows, (((1,), (1,)), ((), ())), preferred_element_type=jnp.float32)
        partial_value = partial_value + lax.dot_general(up_part, up_rows, (((1,), (1,)), ((), ())), preferred_element_type=jnp.float32)
        rounded = lax.optimization_barrier(partial_value.astype(jnp.bfloat16))
        return total + rounded.astype(jnp.float32), None

    start_total = jnp.zeros((tokens.shape[0], tokens.shape[1]), jnp.float32)
    total, unused = lax.scan(add_block, start_total, jnp.arange(N_TP, dtype=jnp.int32))
    input_grad = total.astype(jnp.bfloat16)
    contract = (((0,), (0,)), ((), ()))
    gate_grad = lax.dot_general(tokens, gate_cot, contract, preferred_element_type=jnp.float32)
    up_grad = lax.dot_general(tokens, up_cot, contract, preferred_element_type=jnp.float32)
    down_grad = lax.dot_general(cotangent, hidden, contract, preferred_element_type=jnp.float32)
    return (input_grad, gate_grad, up_grad, down_grad)
```

```python
import functools

import jax
import jax.numpy as jnp
from jax import lax
from jax.experimental import pallas as pl
from jax.experimental.pallas import tpu as pltpu
from jax.sharding import PartitionSpec as P


def row_product(left, right):
    return lax.dot_general(
        left, right, (((1,), (1,)), ((), ())), preferred_element_type=jnp.float32
    )


def token_product(left, right):
    return lax.dot_general(
        left, right, (((0,), (0,)), ((), ())), preferred_element_type=jnp.float32
    )


def owner_sum(received, groups):
    return received.reshape(groups, received.shape[0] // groups, received.shape[1]).sum(axis=0)


def plain_shards(tokens, cotangent, gate_weight, up_weight, down_weight):
    groups = lax.axis_size("fs")
    whole_gate, whole_up, whole_down = (
        lax.all_gather(gate_weight, "fs", axis=0, tiled=True),
        lax.all_gather(up_weight, "fs", axis=0, tiled=True),
        lax.all_gather(down_weight, "fs", axis=0, tiled=True),
    )
    gate = jnp.dot(tokens, whole_gate, preferred_element_type=jnp.float32)
    up = jnp.dot(tokens, whole_up, preferred_element_type=jnp.float32)
    hidden_grad = jnp.dot(cotangent, whole_down, preferred_element_type=jnp.float32)
    sig = jax.nn.sigmoid(gate)
    act = gate * sig
    hidden = (act * up).astype(jnp.bfloat16)
    gate_cot = (hidden_grad * up * sig * (1.0 + gate * (1.0 - sig))).astype(jnp.bfloat16)
    up_cot = (hidden_grad * act).astype(jnp.bfloat16)
    partial_value = row_product(gate_cot, whole_gate) + row_product(up_cot, whole_up)
    input_grad = lax.psum_scatter(
        partial_value.astype(jnp.bfloat16), "tp", scatter_dimension=1, tiled=True
    )
    gate_term = token_product(tokens, gate_cot)
    gate_grad = owner_sum(
        lax.all_to_all(
            gate_term.astype(jnp.bfloat16), "fs", split_axis=0, concat_axis=0, tiled=True
        ).astype(gate_term.dtype),
        groups,
    )
    up_term = token_product(tokens, up_cot)
    up_grad = owner_sum(
        lax.all_to_all(
            up_term.astype(jnp.bfloat16), "fs", split_axis=0, concat_axis=0, tiled=True
        ).astype(up_term.dtype),
        groups,
    )
    down_term = token_product(cotangent, hidden)
    down_grad = owner_sum(
        lax.all_to_all(
            down_term.astype(jnp.bfloat16), "fs", split_axis=0, concat_axis=0, tiled=True
        ).astype(down_term.dtype),
        groups,
    )
    return (input_grad, gate_grad, up_grad, down_grad)


MESH = pl.DeviceIdType.MESH
PARTS = 4
CHIPS = 4
LAG = 7
LAG_OUT = 1
OWN_IN, OWN_OUT = 2, 3
RELAY_IN, RELAY_OUT = 2, 1
GATE, UP, DOWN = 0, 1, 2
RIGHT, LEFT, SIBLING = 0, 1, 2


def kernel(
    n, n_tp, parts, tok, cot, gw, uw, dw, ig_out, gate_out, up_out, down_out,
    x, w_all, acc, cots, own_sum, sib_out, sib_in, line_out, line_in, ig_acc, ig_part, ig_in,
    local_sem, ag_send, ag_recv, sib_send, sib_recv, line_send, line_recv, ig_send, ig_recv,
):
    me, tp = lax.axis_index("fs"), lax.axis_index("tp")
    z, c = me // 2, me % 2
    nz = n // 2
    total = 3 * parts
    other = 2 * z + 1 - c
    rows = gw.shape[1]
    height = gw.shape[0] // parts
    own_columns = ig_out.shape[1]
    pieces = own_columns // rows
    mirrored = z >= nz // 2
    is_end = jnp.logical_or(z == 0, z == nz - 1)
    inward = jnp.where(mirrored, LEFT, RIGHT)
    outward = jnp.where(mirrored, RIGHT, LEFT)

    def chip_at(q):
        return jnp.where(mirrored, nz - 1 - q, q)

    def weight_load(t):
        piece = pl.ds((t // 3) * height, height)
        return pltpu.make_async_copy(
            (gw, uw, dw)[t % 3].at[piece, :], w_all.at[t, me], local_sem.at[t]
        )

    loads = [weight_load(t) for t in range(total)]
    loads += [
        pltpu.make_async_copy(tok, x.at[0], local_sem.at[total]),
        pltpu.make_async_copy(cot, x.at[1], local_sem.at[total + 1]),
    ]
    for load in loads:
        load.start()

    has_left, has_right = z > 0, z < nz - 1
    barrier = pltpu.get_barrier_semaphore()
    pl.semaphore_signal(barrier, inc=1, device_id={"fs": other}, device_id_type=MESH)
    for step in range(1, n_tp):
        pl.semaphore_signal(
            barrier, inc=1, device_id={"tp": lax.rem(tp + step, n_tp)}, device_id_type=MESH
        )

    @pl.when(has_right)
    def _():
        pl.semaphore_signal(barrier, inc=1, device_id={"fs": me + 2}, device_id_type=MESH)

    @pl.when(has_left)
    def _():
        pl.semaphore_signal(barrier, inc=1, device_id={"fs": me - 2}, device_id_type=MESH)

    pl.semaphore_wait(barrier, n_tp + has_left.astype(jnp.int32) + has_right.astype(jnp.int32))

    def line_device(way):
        return me + 2 - 4 * way

    def gather_copy(t, q, way):
        chip = chip_at(q)
        slot = 2 * chip + c
        device = other if way is SIBLING else line_device(way)
        return pltpu.make_async_remote_copy(
            src_ref=w_all.at[t, slot], dst_ref=w_all.at[t, slot],
            send_sem=ag_send.at[t, way, chip], recv_sem=ag_recv.at[t, slot],
            device_id={"fs": device}, device_id_type=MESH,
        )

    def gather_wait(t, q, core):
        slot = 2 * chip_at(q) + core
        pltpu.make_async_remote_copy(
            src_ref=w_all.at[t, slot], dst_ref=w_all.at[t, slot],
            send_sem=ag_send.at[t, SIBLING, 0], recv_sem=ag_recv.at[t, slot],
            device_id={"fs": other}, device_id_type=MESH,
        ).wait_recv()

    def columns_of(slot):
        return pl.ds(pl.multiple_of(slot * rows, rows), rows)

    def pair_product(t, kind, q, first):
        gather_wait(t, q, 1 - c)
        value = None
        for core in range(2):
            slot = 2 * chip_at(q) + core
            part = row_product(w_all[t, slot], x[kind // 2, :, columns_of(slot)])
            value = part if value is None else value + part
        if first:
            acc[kind] = value
        else:
            acc[kind] += value

    def by_rows(body):
        strip = 16

        def step(i, carry):
            body(pl.ds(pl.multiple_of(i * strip, strip), strip))
            return carry

        lax.fori_loop(0, height // strip, step, 0)

    def make_hidden(p):
        t = 3 * p + DOWN

        def strip(r):
            gate = acc[GATE, r, :]
            sig = jax.nn.sigmoid(gate)
            act = gate * sig
            up = acc[UP, r, :]
            cots[t, r, :] = (act * up).astype(jnp.bfloat16)
            acc[UP, r, :] = up * sig * (1.0 + gate * (1.0 - sig))
            acc[GATE, r, :] = act

        by_rows(strip)

    def make_cots(p):
        t = 3 * p

        def strip(r):
            hidden_grad = acc[DOWN, r, :]
            cots[t + GATE, r, :] = (hidden_grad * acc[UP, r, :]).astype(jnp.bfloat16)
            cots[t + UP, r, :] = (hidden_grad * acc[GATE, r, :]).astype(jnp.bfloat16)

        by_rows(strip)

    def side_of(g):
        return lax.rem(g, 3) // 2

    def term(g, slot):
        return jnp.dot(
            cots[g], x[side_of(g), :, columns_of(slot)], preferred_element_type=jnp.float32
        )

    def sibling_copy(g, chip):
        return pltpu.make_async_remote_copy(
            src_ref=sib_out.at[g, chip], dst_ref=sib_in.at[g, chip],
            send_sem=sib_send.at[g, chip], recv_sem=sib_recv.at[g, chip],
            device_id={"fs": other}, device_id_type=MESH,
        )

    def line_copy(g, way, chip):
        return pltpu.make_async_remote_copy(
            src_ref=line_out.at[g, chip], dst_ref=line_in.at[g, way, chip],
            send_sem=line_send.at[g, chip], recv_sem=line_recv.at[g, way, chip],
            device_id={"fs": line_device(way)}, device_id_type=MESH,
        )

    def sibling_terms(g, order):
        for q in order:
            chip = chip_at(q)
            sib_out[g, chip] = term(g, 2 * chip + 1 - c).astype(jnp.bfloat16)
            sibling_copy(g, chip).start()

    def pair_sum(g, chip):
        own = term(g, 2 * chip + c)
        sibling_copy(g, chip).wait_recv()
        return own + sib_in[g, chip].astype(jnp.float32)

    def send_sum(g, q, way, relay):
        chip = chip_at(q)
        value = pair_sum(g, chip)
        if relay:
            line_copy(g, way, chip).wait_recv()
            value = value + line_in[g, way, chip].astype(jnp.float32)
        line_out[g, chip] = value.astype(jnp.bfloat16)
        line_copy(g, way, chip).start()

    def input_copy(peer, source):
        return pltpu.make_async_remote_copy(
            src_ref=ig_part.at[peer], dst_ref=ig_in.at[source],
            send_sem=ig_send.at[peer], recv_sem=ig_recv.at[source],
            device_id={"tp": peer}, device_id_type=MESH,
        )

    def input_terms(p):
        def body(step, carry):
            peer = lax.rem(tp + 1 + step, n_tp)
            value = None
            for t in (3 * p + GATE, 3 * p + UP):
                block = jnp.concatenate(
                    [w_all[t, peer * pieces + i] for i in range(pieces)], axis=1
                )
                part = token_product(cots[t], block)
                value = part if value is None else value + part

            @pl.when(p == 0)
            def _():
                ig_acc[peer] = value

            @pl.when(jnp.logical_and(p > 0, p < parts - 1))
            def _():
                ig_acc[peer] += value

            @pl.when(p == parts - 1)
            def _():
                ig_part[peer] = (ig_acc[peer] + value).astype(jnp.bfloat16)

            @pl.when(jnp.logical_and(p == parts - 1, step < n_tp - 1))
            def _():
                input_copy(peer, tp).start()

            return carry

        lax.fori_loop(0, n_tp, body, 0)

    def end_gather(t, kind):
        gather_wait(t, 1, c)
        gather_copy(t, 1, SIBLING).start()
        pair_product(t, kind, 0, True)
        gather_wait(t, 2, c)
        gather_copy(t, 2, SIBLING).start()
        pair_product(t, kind, 1, False)
        gather_wait(t, 3, c)
        gather_copy(t, 3, SIBLING).start()
        pair_product(t, kind, 2, False)
        pair_product(t, kind, 3, False)

    def end_reduce(low, high):
        def terms(g, carry):
            sibling_terms(g, (3, 2, 1, 0))
            return carry

        def far(g, carry):
            for q in (3, 2):
                send_sum(g, q, inward, False)
            return carry

        def near(g, carry):
            send_sum(g, 1, inward, False)
            own_sum[g] = pair_sum(g, z)
            return carry

        for body in (terms, far, near):
            lax.fori_loop(low, high, body, 0)

    def end_part(p, carry):
        end_gather(3 * p + GATE, GATE)
        end_gather(3 * p + UP, UP)
        make_hidden(p)
        end_reduce(3 * p + DOWN, 3 * p + DOWN + 1)

        @pl.when(p > 0)
        def _():
            input_terms(p - 1)

        end_gather(3 * p + DOWN, DOWN)
        make_cots(p)

        @pl.when(p == parts - 1)
        def _():
            input_terms(p)

        end_reduce(3 * p + GATE, 3 * p + DOWN)
        return carry

    def relay_in(t):
        @pl.when(t < total)
        def _():
            gather_wait(t, 0, c)
            gather_copy(t, 0, inward).start()
            gather_copy(t, 0, SIBLING).start()

        @pl.when(t + OWN_IN < total)
        def _():
            gather_copy(t + OWN_IN, 1, inward).start()

    def relay_near(t):
        @pl.when(t < total)
        def _():
            gather_wait(t, 2, c)
            gather_copy(t, 2, outward).start()
            gather_copy(t, 2, SIBLING).start()

    def relay_far(t):
        @pl.when(t < total)
        def _():
            gather_wait(t, 3, c)
            gather_copy(t, 3, outward).start()
            gather_copy(t, 3, SIBLING).start()

        @pl.when(t + OWN_OUT < total)
        def _():
            gather_copy(t + OWN_OUT, 1, outward).start()

    def middle_gather(t, kind):
        relay_in(t + RELAY_IN)
        pair_product(t, kind, 1, True)
        relay_near(t + RELAY_OUT)
        pair_product(t, kind, 0, False)
        relay_far(t + RELAY_OUT)
        pair_product(t, kind, 2, False)
        pair_product(t, kind, 3, False)

    def in_turn(i):
        return 3 * (i // 3) + lax.rem(i + 2, 3)

    def middle_reduce(r):
        @pl.when(jnp.logical_and(r >= -1, r < total - 1))
        def _():
            sibling_terms(in_turn(r + 1), (3, 2, 0, 1))

        @pl.when(jnp.logical_and(r >= 0, r < total))
        def _():
            g = in_turn(r)
            send_sum(g, 3, inward, True)
            send_sum(g, 2, inward, True)
            own_sum[g] = pair_sum(g, z)

        @pl.when(r >= LAG_OUT)
        def _():
            send_sum(in_turn(r - LAG_OUT), 0, outward, True)

    def middle_part(p, carry):
        for kind in (GATE, UP, DOWN):
            t = 3 * p + kind
            middle_gather(t, kind)
            if kind == UP:
                make_hidden(p)
            if kind == DOWN:
                make_cots(p)
            middle_reduce(t - LAG)
        input_terms(p)
        return carry

    def middle_rest(r, carry):
        middle_reduce(r)
        return carry

    for t in range(total):
        loads[t].wait()
        gather_copy(t, jnp.where(is_end, 0, 1), SIBLING).start()

        @pl.when(is_end)
        def _():
            gather_copy(t, 0, inward).start()

        if t < OWN_OUT:
            @pl.when(jnp.logical_not(is_end))
            def _():
                gather_copy(t, 1, outward).start()

        if t < OWN_IN:
            @pl.when(jnp.logical_not(is_end))
            def _():
                gather_copy(t, 1, inward).start()

    loads[total].wait()
    loads[total + 1].wait()

    @pl.when(is_end)
    def _():
        lax.fori_loop(0, parts, end_part, 0)

    @pl.when(jnp.logical_not(is_end))
    def _():
        for t in range(RELAY_IN):
            relay_in(t)
        for t in range(RELAY_OUT):
            relay_near(t)
            relay_far(t)
        lax.fori_loop(0, parts, middle_part, 0)
        lax.fori_loop(total - LAG, total + LAG_OUT, middle_rest, 0)

    ig_in[tp] = ig_part[tp]
    for step in range(1, n_tp):
        source = lax.rem(tp + step, n_tp)
        input_copy(source, source).wait_recv()
    for half in range(2):
        strip = ig_out.shape[0] // 2
        r = pl.ds(half * strip, strip)
        value = ig_in[0, r, :].astype(jnp.float32)
        for source in range(1, n_tp):
            value = value + ig_in[source, r, :].astype(jnp.float32)
        ig_out[r, :] = value.astype(ig_out.dtype)

    for p in range(parts):
        for kind in (DOWN, GATE, UP):
            g = 3 * p + kind
            piece = pl.ds(p * height, height)
            out = (gate_out, up_out, down_out)[kind]
            line_copy(g, outward, z).wait_recv()
            value = own_sum[g] + line_in[g, outward, z].astype(jnp.float32)
            out[piece, :] = value

            @pl.when(jnp.logical_not(is_end))
            def _():
                line_copy(g, inward, z).wait_recv()
                out[piece, :] += line_in[g, inward, z].astype(jnp.float32)

    def drain(g, carry):
        for chip in range(nz):
            gather_copy(g, chip, SIBLING).wait_send()
            sibling_copy(g, chip).wait_send()

            @pl.when(chip != z)
            def _():
                way = jnp.where(chip > z, RIGHT, LEFT)
                line_copy(g, way, chip).wait_send()

            @pl.when(jnp.logical_and(has_right, chip <= z))
            def _():
                absolute_copy(g, chip, RIGHT).wait_send()

            @pl.when(jnp.logical_and(has_left, chip >= z))
            def _():
                absolute_copy(g, chip, LEFT).wait_send()

        return carry

    def absolute_copy(t, chip, way):
        slot = 2 * chip + c
        return pltpu.make_async_remote_copy(
            src_ref=w_all.at[t, slot], dst_ref=w_all.at[t, slot],
            send_sem=ag_send.at[t, way, chip], recv_sem=ag_recv.at[t, slot],
            device_id={"fs": line_device(way)}, device_id_type=MESH,
        )

    lax.fori_loop(0, total, drain, 0)
    for step in range(1, n_tp):
        input_copy(lax.rem(tp + step, n_tp), tp).wait_send()


def fused_shards(tokens, cotangent, gate_weight, up_weight, down_weight):
    n, n_tp = lax.axis_size("fs"), lax.axis_size("tp")
    nz = n // 2
    count, width = tokens.shape
    rows, hidden = gate_weight.shape
    height = hidden // PARTS
    pieces = 3 * PARTS
    share = width // n_tp
    bf16, f32 = jnp.bfloat16, jnp.float32
    dma = pltpu.SemaphoreType.DMA
    input_grad, gate_grad, up_grad, down_grad = pl.pallas_call(
        functools.partial(kernel, n, n_tp, PARTS),
        out_shape=(
            jax.ShapeDtypeStruct((count, share), bf16),
        ) + (jax.ShapeDtypeStruct((hidden, rows), f32),) * 3,
        in_specs=[pl.BlockSpec(memory_space=pl.ANY)] * 5,
        out_specs=(pl.BlockSpec(memory_space=pltpu.VMEM),) * 4,
        scratch_shapes=[
            pltpu.VMEM((2, count, width), bf16),
            pltpu.VMEM((pieces, n, height, rows), bf16),
            pltpu.VMEM((3, height, count), f32),
            pltpu.VMEM((pieces, height, count), bf16),
            pltpu.VMEM((pieces, height, rows), f32),
            pltpu.VMEM((pieces, nz, height, rows), bf16),
            pltpu.VMEM((pieces, nz, height, rows), bf16),
            pltpu.VMEM((pieces, nz, height, rows), bf16),
            pltpu.VMEM((pieces, 2, nz, height, rows), bf16),
            pltpu.VMEM((n_tp, count, share), f32),
            pltpu.VMEM((n_tp, count, share), bf16),
            pltpu.VMEM((n_tp, count, share), bf16),
            dma((pieces + 2,)),
            dma((pieces, 3, nz)),
            dma((pieces, n)),
            dma((pieces, nz)),
            dma((pieces, nz)),
            dma((pieces, nz)),
            dma((pieces, 2, nz)),
            dma((n_tp,)),
            dma((n_tp,)),
        ],
        compiler_params=pltpu.CompilerParams(
            collective_id=0, has_side_effects=True, vmem_limit_bytes=67043328
        ),
    )(tokens, cotangent, gate_weight.T, up_weight.T, down_weight.T)
    return input_grad, gate_grad.T, up_grad.T, down_grad.T


def shards(tokens, cotangent, gate_weight, up_weight, down_weight):
    n, n_tp = lax.axis_size("fs"), lax.axis_size("tp")
    rows = gate_weight.shape[0]
    share = tokens.shape[1] // n_tp
    if n == 2 * CHIPS and rows % 128 == 0 and share % rows == 0 and (
        gate_weight.shape[1] % (16 * PARTS) == 0
    ):
        return fused_shards(tokens, cotangent, gate_weight, up_weight, down_weight)
    return plain_shards(tokens, cotangent, gate_weight, up_weight, down_weight)


def solution(mesh):
    in_specs = (P("fs", None), P("fs", None), P("fs", "tp"), P("fs", "tp"), P("fs", "tp"))
    out_specs = (P("fs", "tp"), P("fs", "tp"), P("fs", "tp"), P("fs", "tp"))
    return jax.shard_map(shards, mesh=mesh, in_specs=in_specs, out_specs=out_specs, check_vma=False)
```

```python
import functools

import jax
import jax.numpy as jnp
from jax import lax
from jax.experimental import pallas as pl
from jax.experimental.pallas import tpu as pltpu
from jax.sharding import PartitionSpec as P


def row_product(left, right):
    return lax.dot_general(
        left, right, (((1,), (1,)), ((), ())), preferred_element_type=jnp.float32
    )


def token_product(left, right):
    return lax.dot_general(
        left, right, (((0,), (0,)), ((), ())), preferred_element_type=jnp.float32
    )


def owner_sum(received, groups):
    return received.reshape(groups, received.shape[0] // groups, received.shape[1]).sum(axis=0)


def plain_shards(tokens, cotangent, gate_weight, up_weight, down_weight):
    groups = lax.axis_size("fs")
    whole_gate, whole_up, whole_down = (
        lax.all_gather(gate_weight, "fs", axis=0, tiled=True),
        lax.all_gather(up_weight, "fs", axis=0, tiled=True),
        lax.all_gather(down_weight, "fs", axis=0, tiled=True),
    )
    gate = jnp.dot(tokens, whole_gate, preferred_element_type=jnp.float32)
    up = jnp.dot(tokens, whole_up, preferred_element_type=jnp.float32)
    hidden_grad = jnp.dot(cotangent, whole_down, preferred_element_type=jnp.float32)
    sig = jax.nn.sigmoid(gate)
    act = gate * sig
    hidden = (act * up).astype(jnp.bfloat16)
    gate_cot = (hidden_grad * up * sig * (1.0 + gate * (1.0 - sig))).astype(jnp.bfloat16)
    up_cot = (hidden_grad * act).astype(jnp.bfloat16)
    partial_value = row_product(gate_cot, whole_gate) + row_product(up_cot, whole_up)
    input_grad = lax.psum_scatter(
        partial_value.astype(jnp.bfloat16), "tp", scatter_dimension=1, tiled=True
    )
    gate_term = token_product(tokens, gate_cot)
    gate_grad = owner_sum(
        lax.all_to_all(
            gate_term.astype(jnp.bfloat16), "fs", split_axis=0, concat_axis=0, tiled=True
        ).astype(gate_term.dtype),
        groups,
    )
    up_term = token_product(tokens, up_cot)
    up_grad = owner_sum(
        lax.all_to_all(
            up_term.astype(jnp.bfloat16), "fs", split_axis=0, concat_axis=0, tiled=True
        ).astype(up_term.dtype),
        groups,
    )
    down_term = token_product(cotangent, hidden)
    down_grad = owner_sum(
        lax.all_to_all(
            down_term.astype(jnp.bfloat16), "fs", split_axis=0, concat_axis=0, tiled=True
        ).astype(down_term.dtype),
        groups,
    )
    return (input_grad, gate_grad, up_grad, down_grad)


MESH = pl.DeviceIdType.MESH
PARTS = 4
CHIPS = 4
LAG = 7
VMEM_BYTES = 56 * 1024 * 1024
DELIVER_BYTES = 1024 * 1024
LAG_OUT = 1
LAG_FINAL = 4
INPUT_TURN = 3
OWN_IN, OWN_OUT = 2, 3
RELAY_IN, RELAY_OUT = 2, 1
GATE, UP, DOWN = 0, 1, 2
RIGHT, LEFT, SIBLING = 0, 1, 2


def kernel(
    n, n_tp, parts, tok, cot, gw, uw, dw, ig_out, own_sum,
    x, w_all, acc, cots, sib_out, sib_in, line_out, line_in, ig_acc, ig_part, ig_in, ig_mid,
    local_sem, ag_send, ag_recv, sib_send, sib_recv, line_send, line_recv, ig_send, ig_recv,
):
    me, tp = lax.axis_index("fs"), lax.axis_index("tp")
    z, c = me // 2, me % 2
    nz = n // 2
    total = 3 * parts
    other = 2 * z + 1 - c
    rows = gw.shape[1]
    height = gw.shape[0] // parts
    own_columns = ig_out.shape[1]
    pieces = own_columns // rows
    mirrored = z >= nz // 2
    is_end = jnp.logical_or(z == 0, z == nz - 1)
    inward = jnp.where(mirrored, LEFT, RIGHT)
    outward = jnp.where(mirrored, RIGHT, LEFT)

    def chip_at(q):
        return jnp.where(mirrored, nz - 1 - q, q)

    def weight_load(t):
        piece = pl.ds((t // 3) * height, height)
        return pltpu.make_async_copy(
            (gw, uw, dw)[t % 3].at[piece, :], w_all.at[t, me], local_sem.at[t]
        )

    loads = [weight_load(t) for t in range(total)]
    loads += [
        pltpu.make_async_copy(tok, x.at[0], local_sem.at[total]),
        pltpu.make_async_copy(cot, x.at[1], local_sem.at[total + 1]),
    ]
    for load in loads:
        load.start()

    has_left, has_right = z > 0, z < nz - 1
    barrier = pltpu.get_barrier_semaphore()
    pl.semaphore_signal(barrier, inc=1, device_id={"fs": other}, device_id_type=MESH)
    for step in range(1, n_tp):
        pl.semaphore_signal(
            barrier, inc=1, device_id={"tp": lax.rem(tp + step, n_tp)}, device_id_type=MESH
        )

    @pl.when(has_right)
    def _():
        pl.semaphore_signal(barrier, inc=1, device_id={"fs": me + 2}, device_id_type=MESH)

    @pl.when(has_left)
    def _():
        pl.semaphore_signal(barrier, inc=1, device_id={"fs": me - 2}, device_id_type=MESH)

    pl.semaphore_wait(barrier, n_tp + has_left.astype(jnp.int32) + has_right.astype(jnp.int32))

    def line_device(way):
        return me + 2 - 4 * way

    def gather_copy(t, q, way):
        chip = chip_at(q)
        slot = 2 * chip + c
        device = other if way is SIBLING else line_device(way)
        return pltpu.make_async_remote_copy(
            src_ref=w_all.at[t, slot], dst_ref=w_all.at[t, slot],
            send_sem=ag_send.at[t, way, chip], recv_sem=ag_recv.at[t, slot],
            device_id={"fs": device}, device_id_type=MESH,
        )

    def gather_wait(t, q, core):
        slot = 2 * chip_at(q) + core
        pltpu.make_async_remote_copy(
            src_ref=w_all.at[t, slot], dst_ref=w_all.at[t, slot],
            send_sem=ag_send.at[t, SIBLING, 0], recv_sem=ag_recv.at[t, slot],
            device_id={"fs": other}, device_id_type=MESH,
        ).wait_recv()

    def columns_of(slot):
        return pl.ds(pl.multiple_of(slot * rows, rows), rows)

    def pair_product(t, kind, q, first):
        gather_wait(t, q, 1 - c)
        value = None
        for core in range(2):
            slot = 2 * chip_at(q) + core
            part = row_product(w_all[t, slot], x[kind // 2, :, columns_of(slot)])
            value = part if value is None else value + part
        if first:
            acc[kind] = value
        else:
            acc[kind] += value

    def by_rows(body):
        strip = 16

        def step(i, carry):
            body(pl.ds(pl.multiple_of(i * strip, strip), strip))
            return carry

        lax.fori_loop(0, height // strip, step, 0)

    def make_hidden(p):
        t = 3 * p + DOWN

        def strip(r):
            gate = acc[GATE, r, :]
            sig = jax.nn.sigmoid(gate)
            act = gate * sig
            up = acc[UP, r, :]
            cots[t, r, :] = (act * up).astype(jnp.bfloat16)
            acc[UP, r, :] = up * sig * (1.0 + gate * (1.0 - sig))
            acc[GATE, r, :] = act

        by_rows(strip)

    def make_cots(p):
        t = 3 * p

        def strip(r):
            hidden_grad = acc[DOWN, r, :]
            cots[t + GATE, r, :] = (hidden_grad * acc[UP, r, :]).astype(jnp.bfloat16)
            cots[t + UP, r, :] = (hidden_grad * acc[GATE, r, :]).astype(jnp.bfloat16)

        by_rows(strip)

    def side_of(g):
        return lax.rem(g, 3) // 2

    def term(g, slot):
        return jnp.dot(
            cots[g], x[side_of(g), :, columns_of(slot)], preferred_element_type=jnp.float32
        )

    def sibling_copy(g, chip):
        return pltpu.make_async_remote_copy(
            src_ref=sib_out.at[g, chip], dst_ref=sib_in.at[g, chip],
            send_sem=sib_send.at[g, chip], recv_sem=sib_recv.at[g, chip],
            device_id={"fs": other}, device_id_type=MESH,
        )

    def line_copy(g, way, chip):
        return pltpu.make_async_remote_copy(
            src_ref=line_out.at[g, chip], dst_ref=line_in.at[g, way, chip],
            send_sem=line_send.at[g, chip], recv_sem=line_recv.at[g, way, chip],
            device_id={"fs": line_device(way)}, device_id_type=MESH,
        )

    def sibling_terms(g, order):
        for q in order:
            chip = chip_at(q)
            sib_out[g, chip] = term(g, 2 * chip + 1 - c).astype(jnp.bfloat16)
            sibling_copy(g, chip).start()

    def pair_sum(g, chip):
        own = term(g, 2 * chip + c)
        sibling_copy(g, chip).wait_recv()
        return own + sib_in[g, chip].astype(jnp.float32)

    def send_sum(g, q, way, relay):
        chip = chip_at(q)
        value = pair_sum(g, chip)
        if relay:
            line_copy(g, way, chip).wait_recv()
            value = value + line_in[g, way, chip].astype(jnp.float32)
        line_out[g, chip] = value.astype(jnp.bfloat16)
        line_copy(g, way, chip).start()

    side_peer = tp + 1 - 2 * lax.rem(tp, 2)
    far_peer = lax.rem(tp + 2, n_tp)
    corner = lax.rem(side_peer + 2, n_tp)
    half = ig_out.shape[0] // 2

    def half_rows(s):
        return pl.ds(s * half, half)

    def input_copy(k, source):
        s = k % 2
        peers = (side_peer, far_peer) if k < 4 else (far_peer, side_peer)
        return pltpu.make_async_remote_copy(
            src_ref=source, dst_ref=ig_in.at[k], send_sem=ig_send.at[k], recv_sem=ig_recv.at[k],
            device_id={"tp": peers[s]}, device_id_type=MESH,
        )

    def corner_copy(s):
        return input_copy(s, ig_part.at[corner, half_rows(s), :])

    def direct_copy(s):
        return input_copy(2 + s, ig_part.at[(side_peer, far_peer)[s], half_rows(s), :])

    def relay_copy(s):
        return input_copy(4 + s, ig_mid.at[s])

    def input_relay():
        for s in range(2):
            corner_copy(s).wait_recv()
            own = ig_part[(far_peer, side_peer)[s], half_rows(s), :].astype(jnp.float32)
            ig_mid[s] = (own + ig_in[s].astype(jnp.float32)).astype(jnp.bfloat16)
            relay_copy(s).start()

    def input_terms(p):
        def body(step, carry):
            peer = jnp.where(
                step == 0, corner, jnp.where(step == 1, side_peer, jnp.where(step == 2, far_peer, tp))
            )
            value = None
            for t in (3 * p + GATE, 3 * p + UP):
                block = jnp.concatenate(
                    [w_all[t, peer * pieces + i] for i in range(pieces)], axis=1
                )
                part = token_product(cots[t], block)
                value = part if value is None else value + part

            @pl.when(p == 0)
            def _():
                ig_acc[peer] = value

            @pl.when(jnp.logical_and(p > 0, p < parts - 1))
            def _():
                ig_acc[peer] += value

            @pl.when(p == parts - 1)
            def _():
                ig_part[peer] = (ig_acc[peer] + value).astype(jnp.bfloat16)

            @pl.when(jnp.logical_and(p == parts - 1, step == 0))
            def _():
                corner_copy(0).start()
                corner_copy(1).start()

            @pl.when(jnp.logical_and(p == parts - 1, step == 1))
            def _():
                direct_copy(0).start()

            @pl.when(jnp.logical_and(p == parts - 1, step == 2))
            def _():
                direct_copy(1).start()

            return carry

        lax.fori_loop(0, n_tp, body, 0)

    def end_gather(t, kind):
        gather_wait(t, 1, c)
        gather_copy(t, 1, SIBLING).start()
        pair_product(t, kind, 0, True)
        gather_wait(t, 2, c)
        gather_copy(t, 2, SIBLING).start()
        pair_product(t, kind, 1, False)
        gather_wait(t, 3, c)
        gather_copy(t, 3, SIBLING).start()
        pair_product(t, kind, 2, False)
        pair_product(t, kind, 3, False)

    def end_reduce(low, high):
        def terms(g, carry):
            sibling_terms(g, (3, 2, 1, 0))
            return carry

        def far(g, carry):
            for q in (3, 2):
                send_sum(g, q, inward, False)
            return carry

        def near(g, carry):
            send_sum(g, 1, inward, False)
            own_sum[g] = pair_sum(g, z)
            return carry

        for body in (terms, far, near):
            lax.fori_loop(low, high, body, 0)

    def end_part(p, carry):
        end_gather(3 * p + GATE, GATE)
        end_gather(3 * p + UP, UP)
        make_hidden(p)
        end_reduce(3 * p + DOWN, 3 * p + DOWN + 1)

        @pl.when(p > 0)
        def _():
            input_terms(p - 1)

        end_gather(3 * p + DOWN, DOWN)
        make_cots(p)

        @pl.when(p == parts - 1)
        def _():
            input_terms(p)

        end_reduce(3 * p + GATE, 3 * p + DOWN)
        return carry

    def relay_in(t):
        @pl.when(t < total)
        def _():
            gather_wait(t, 0, c)
            gather_copy(t, 0, inward).start()
            gather_copy(t, 0, SIBLING).start()

        @pl.when(t + OWN_IN < total)
        def _():
            gather_copy(t + OWN_IN, 1, inward).start()

    def relay_near(t):
        @pl.when(t < total)
        def _():
            gather_wait(t, 2, c)
            gather_copy(t, 2, outward).start()
            gather_copy(t, 2, SIBLING).start()

    def relay_far(t):
        @pl.when(t < total)
        def _():
            gather_wait(t, 3, c)
            gather_copy(t, 3, outward).start()
            gather_copy(t, 3, SIBLING).start()

        @pl.when(t + OWN_OUT < total)
        def _():
            gather_copy(t + OWN_OUT, 1, outward).start()

    def middle_gather(t, kind):
        relay_in(t + RELAY_IN)
        pair_product(t, kind, 1, True)
        relay_near(t + RELAY_OUT)
        pair_product(t, kind, 0, False)
        relay_far(t + RELAY_OUT)
        pair_product(t, kind, 2, False)
        pair_product(t, kind, 3, False)

    def in_turn(i):
        return 3 * (i // 3) + lax.rem(i + 2, 3)

    def final(r, carry):
        g = in_turn(r)
        line_copy(g, outward, z).wait_recv()
        own_sum[g] += line_in[g, outward, z].astype(jnp.float32)
        return carry

    def middle_final(r, carry):
        g = in_turn(r)
        for way in (inward, outward):
            line_copy(g, way, z).wait_recv()
        own_sum[g] += (
            line_in[g, inward, z].astype(jnp.float32) + line_in[g, outward, z].astype(jnp.float32)
        )
        return carry

    def middle_reduce(r):
        @pl.when(jnp.logical_and(r >= -1, r < total - 1))
        def _():
            sibling_terms(in_turn(r + 1), (3, 2, 0, 1))

        @pl.when(jnp.logical_and(r >= 0, r < total))
        def _():
            g = in_turn(r)
            send_sum(g, 3, inward, True)
            send_sum(g, 2, inward, True)
            own_sum[g] = pair_sum(g, z)

        @pl.when(r >= LAG_OUT)
        def _():
            send_sum(in_turn(r - LAG_OUT), 0, outward, True)

        @pl.when(r >= LAG_FINAL)
        def _():
            middle_final(r - LAG_FINAL, 0)

    def middle_part(p, carry):
        for kind in (GATE, UP, DOWN):
            t = 3 * p + kind
            middle_gather(t, kind)
            if kind == UP:
                make_hidden(p)
            if kind == DOWN:
                make_cots(p)
            middle_reduce(t - LAG)
        input_terms(p)
        return carry

    def middle_rest(r, carry):
        middle_reduce(r)

        @pl.when(r == total - INPUT_TURN)
        def _():
            input_relay()

        return carry

    for t in range(total):
        loads[t].wait()
        gather_copy(t, jnp.where(is_end, 0, 1), SIBLING).start()

        @pl.when(is_end)
        def _():
            gather_copy(t, 0, inward).start()

        if t < OWN_OUT:
            @pl.when(jnp.logical_not(is_end))
            def _():
                gather_copy(t, 1, outward).start()

        if t < OWN_IN:
            @pl.when(jnp.logical_not(is_end))
            def _():
                gather_copy(t, 1, inward).start()

    loads[total].wait()
    loads[total + 1].wait()

    @pl.when(is_end)
    def _():
        lax.fori_loop(0, parts, end_part, 0)
        input_relay()
        lax.fori_loop(0, total, final, 0)

    @pl.when(jnp.logical_not(is_end))
    def _():
        for t in range(RELAY_IN):
            relay_in(t)
        for t in range(RELAY_OUT):
            relay_near(t)
            relay_far(t)
        lax.fori_loop(0, parts, middle_part, 0)
        lax.fori_loop(total - LAG, total + LAG_OUT, middle_rest, 0)
        lax.fori_loop(total + LAG_OUT - LAG_FINAL, total, middle_final, 0)

    for s in range(2):
        direct_copy(s).wait_recv()
        relay_copy(s).wait_recv()
        value = ig_part[tp, half_rows(s), :].astype(jnp.float32)
        for k in (2 + s, 4 + s):
            value = value + ig_in[k].astype(jnp.float32)
        ig_out[half_rows(s), :] = value.astype(ig_out.dtype)

    def drain(g, carry):
        for chip in range(nz):
            gather_copy(g, chip, SIBLING).wait_send()
            sibling_copy(g, chip).wait_send()

            @pl.when(chip != z)
            def _():
                way = jnp.where(chip > z, RIGHT, LEFT)
                line_copy(g, way, chip).wait_send()

            @pl.when(jnp.logical_and(has_right, chip <= z))
            def _():
                absolute_copy(g, chip, RIGHT).wait_send()

            @pl.when(jnp.logical_and(has_left, chip >= z))
            def _():
                absolute_copy(g, chip, LEFT).wait_send()

        return carry

    def absolute_copy(t, chip, way):
        slot = 2 * chip + c
        return pltpu.make_async_remote_copy(
            src_ref=w_all.at[t, slot], dst_ref=w_all.at[t, slot],
            send_sem=ag_send.at[t, way, chip], recv_sem=ag_recv.at[t, slot],
            device_id={"fs": line_device(way)}, device_id_type=MESH,
        )

    lax.fori_loop(0, total, drain, 0)
    for s in range(2):
        for copy in (corner_copy, direct_copy, relay_copy):
            copy(s).wait_send()


def fused_shards(tokens, cotangent, gate_weight, up_weight, down_weight):
    n, n_tp = lax.axis_size("fs"), lax.axis_size("tp")
    nz = n // 2
    count, width = tokens.shape
    rows, hidden = gate_weight.shape
    height = hidden // PARTS
    pieces = 3 * PARTS
    share = width // n_tp
    bf16, f32 = jnp.bfloat16, jnp.float32
    dma = pltpu.SemaphoreType.DMA
    input_grad, sums = pl.pallas_call(
        functools.partial(kernel, n, n_tp, PARTS),
        out_shape=(pltpu.VMEM((count, share), bf16), pltpu.VMEM((pieces, height, rows), f32)),
        in_specs=[pl.BlockSpec(memory_space=pl.ANY)] * 5,
        out_specs=(pl.BlockSpec(memory_space=pltpu.VMEM),) * 2,
        scratch_shapes=[
            pltpu.VMEM((2, count, width), bf16),
            pltpu.VMEM((pieces, n, height, rows), bf16),
            pltpu.VMEM((3, height, count), f32),
            pltpu.VMEM((pieces, height, count), bf16),
            pltpu.VMEM((pieces, nz, height, rows), bf16),
            pltpu.VMEM((pieces, nz, height, rows), bf16),
            pltpu.VMEM((pieces, nz, height, rows), bf16),
            pltpu.VMEM((pieces, 2, nz, height, rows), bf16),
            pltpu.VMEM((n_tp, count, share), f32),
            pltpu.VMEM((n_tp, count, share), bf16),
            pltpu.VMEM((6, count // 2, share), bf16),
            pltpu.VMEM((2, count // 2, share), bf16),
            dma((pieces + 2,)),
            dma((pieces, 3, nz)),
            dma((pieces, n)),
            dma((pieces, nz)),
            dma((pieces, nz)),
            dma((pieces, nz)),
            dma((pieces, 2, nz)),
            dma((6,)),
            dma((6,)),
        ],
        compiler_params=pltpu.CompilerParams(
            collective_id=0, has_side_effects=True, vmem_limit_bytes=VMEM_BYTES
        ),
    )(tokens, cotangent, gate_weight.T, up_weight.T, down_weight.T)
    input_grad, gate_grad, up_grad, down_grad = pl.pallas_call(
        functools.partial(deliver, PARTS),
        out_shape=(
            jax.ShapeDtypeStruct((count, share), bf16),
        ) + (jax.ShapeDtypeStruct((hidden, rows), f32),) * 3,
        in_specs=[pl.BlockSpec(memory_space=pltpu.VMEM)] * 2,
        out_specs=(pl.BlockSpec(memory_space=pl.ANY),) * 4,
        scratch_shapes=[dma((pieces + 1,))],
        compiler_params=pltpu.CompilerParams(vmem_limit_bytes=DELIVER_BYTES),
    )(*(pltpu.with_memory_space_constraint(v, pltpu.VMEM) for v in (input_grad, sums)))
    return input_grad, gate_grad.T, up_grad.T, down_grad.T


def deliver(parts, ig, sums, ig_out, gate_out, up_out, down_out, sem):
    height = sums.shape[1]
    copies = [pltpu.make_async_copy(ig, ig_out, sem.at[3 * parts])]
    for g in range(3 * parts):
        out = (gate_out, up_out, down_out)[g % 3]
        piece = pl.ds((g // 3) * height, height)
        copies.append(pltpu.make_async_copy(sums.at[g], out.at[piece, :], sem.at[g]))
    for copy in copies:
        copy.start()
    for copy in copies:
        copy.wait()


def shards(tokens, cotangent, gate_weight, up_weight, down_weight):
    n, n_tp = lax.axis_size("fs"), lax.axis_size("tp")
    rows = gate_weight.shape[0]
    share = tokens.shape[1] // n_tp
    if n == 2 * CHIPS and n_tp == 4 and rows % 128 == 0 and share % rows == 0 and (
        gate_weight.shape[1] % (16 * PARTS) == 0
    ):
        return fused_shards(tokens, cotangent, gate_weight, up_weight, down_weight)
    return plain_shards(tokens, cotangent, gate_weight, up_weight, down_weight)


def solution(mesh):
    in_specs = (P("fs", None), P("fs", None), P("fs", "tp"), P("fs", "tp"), P("fs", "tp"))
    out_specs = (P("fs", "tp"), P("fs", "tp"), P("fs", "tp"), P("fs", "tp"))
    return jax.shard_map(shards, mesh=mesh, in_specs=in_specs, out_specs=out_specs, check_vma=False)
```

```python
import functools

import jax
import jax.numpy as jnp
from jax import lax
from jax.experimental import pallas as pl
from jax.experimental.pallas import tpu as pltpu
from jax.sharding import PartitionSpec as P


def row_product(left, right):
    return lax.dot_general(
        left, right, (((1,), (1,)), ((), ())), preferred_element_type=jnp.float32
    )


def token_product(left, right):
    return lax.dot_general(
        left, right, (((0,), (0,)), ((), ())), preferred_element_type=jnp.float32
    )


def owner_sum(received, groups):
    return received.reshape(groups, received.shape[0] // groups, received.shape[1]).sum(axis=0)


def plain_shards(tokens, cotangent, gate_weight, up_weight, down_weight):
    groups = lax.axis_size("fs")
    whole_gate, whole_up, whole_down = (
        lax.all_gather(gate_weight, "fs", axis=0, tiled=True),
        lax.all_gather(up_weight, "fs", axis=0, tiled=True),
        lax.all_gather(down_weight, "fs", axis=0, tiled=True),
    )
    gate = jnp.dot(tokens, whole_gate, preferred_element_type=jnp.float32)
    up = jnp.dot(tokens, whole_up, preferred_element_type=jnp.float32)
    hidden_grad = jnp.dot(cotangent, whole_down, preferred_element_type=jnp.float32)
    sig = jax.nn.sigmoid(gate)
    act = gate * sig
    hidden = (act * up).astype(jnp.bfloat16)
    gate_cot = (hidden_grad * up * sig * (1.0 + gate * (1.0 - sig))).astype(jnp.bfloat16)
    up_cot = (hidden_grad * act).astype(jnp.bfloat16)
    partial_value = row_product(gate_cot, whole_gate) + row_product(up_cot, whole_up)
    input_grad = lax.psum_scatter(
        partial_value.astype(jnp.bfloat16), "tp", scatter_dimension=1, tiled=True
    )
    gate_term = token_product(tokens, gate_cot)
    gate_grad = owner_sum(
        lax.all_to_all(
            gate_term.astype(jnp.bfloat16), "fs", split_axis=0, concat_axis=0, tiled=True
        ).astype(gate_term.dtype),
        groups,
    )
    up_term = token_product(tokens, up_cot)
    up_grad = owner_sum(
        lax.all_to_all(
            up_term.astype(jnp.bfloat16), "fs", split_axis=0, concat_axis=0, tiled=True
        ).astype(up_term.dtype),
        groups,
    )
    down_term = token_product(cotangent, hidden)
    down_grad = owner_sum(
        lax.all_to_all(
            down_term.astype(jnp.bfloat16), "fs", split_axis=0, concat_axis=0, tiled=True
        ).astype(down_term.dtype),
        groups,
    )
    return (input_grad, gate_grad, up_grad, down_grad)


MESH = pl.DeviceIdType.MESH
PARTS = 4
CHIPS = 4
LAG = 7
VMEM_BYTES = 60 * 1024 * 1024
DELIVER_BYTES = 1024 * 1024
LAG_OUT, LAG_NEAR, LAG_FINAL = 2, 1, 5
INPUT_TURN = 5
OWN_IN, OWN_OUT = 2, 3
RELAY_IN, RELAY_OUT = 2, 1
GATE, UP, DOWN = 0, 1, 2
RIGHT, LEFT, SIBLING = 0, 1, 2


def kernel(
    n, n_tp, parts, tok, cot, gw, uw, dw, ig_out, own_sum,
    x, w_all, acc, cots, cots_turned, own_term, sib_out, sib_in, line_out, line_in, ig_acc, ig_part, ig_in, ig_mid,
    local_sem, ag_send, ag_recv, sib_send, sib_recv, line_send, line_recv, ig_send, ig_recv,
):
    me, tp = lax.axis_index("fs"), lax.axis_index("tp")
    z, c = me // 2, me % 2
    nz = n // 2
    total = 3 * parts
    other = 2 * z + 1 - c
    rows = gw.shape[1]
    height = gw.shape[0] // parts
    own_columns = ig_out.shape[1]
    pieces = own_columns // rows
    mirrored = z >= nz // 2
    is_end = jnp.logical_or(z == 0, z == nz - 1)
    inward = jnp.where(mirrored, LEFT, RIGHT)
    outward = jnp.where(mirrored, RIGHT, LEFT)

    def chip_at(q):
        return jnp.where(mirrored, nz - 1 - q, q)

    def weight_load(t):
        piece = pl.ds((t // 3) * height, height)
        return pltpu.make_async_copy(
            (gw, uw, dw)[t % 3].at[piece, :], w_all.at[t, me], local_sem.at[t]
        )

    loads = [weight_load(t) for t in range(total)]
    loads += [
        pltpu.make_async_copy(tok, x.at[0], local_sem.at[total]),
        pltpu.make_async_copy(cot, x.at[1], local_sem.at[total + 1]),
    ]
    for load in loads:
        load.start()

    has_left, has_right = z > 0, z < nz - 1
    barrier = pltpu.get_barrier_semaphore()
    pl.semaphore_signal(barrier, inc=1, device_id={"fs": other}, device_id_type=MESH)
    for step in range(1, n_tp):
        pl.semaphore_signal(
            barrier, inc=1, device_id={"tp": lax.rem(tp + step, n_tp)}, device_id_type=MESH
        )

    @pl.when(has_right)
    def _():
        pl.semaphore_signal(barrier, inc=1, device_id={"fs": me + 2}, device_id_type=MESH)

    @pl.when(has_left)
    def _():
        pl.semaphore_signal(barrier, inc=1, device_id={"fs": me - 2}, device_id_type=MESH)

    pl.semaphore_wait(barrier, n_tp + has_left.astype(jnp.int32) + has_right.astype(jnp.int32))

    def line_device(way):
        return me + 2 - 4 * way

    def gather_copy(t, q, way):
        chip = chip_at(q)
        slot = 2 * chip + c
        device = other if way is SIBLING else line_device(way)
        return pltpu.make_async_remote_copy(
            src_ref=w_all.at[t, slot], dst_ref=w_all.at[t, slot],
            send_sem=ag_send.at[t, way, chip], recv_sem=ag_recv.at[t, slot],
            device_id={"fs": device}, device_id_type=MESH,
        )

    def gather_wait(t, q, core):
        slot = 2 * chip_at(q) + core
        pltpu.make_async_remote_copy(
            src_ref=w_all.at[t, slot], dst_ref=w_all.at[t, slot],
            send_sem=ag_send.at[t, SIBLING, 0], recv_sem=ag_recv.at[t, slot],
            device_id={"fs": other}, device_id_type=MESH,
        ).wait_recv()

    def columns_of(slot):
        return pl.ds(pl.multiple_of(slot * rows, rows), rows)

    def pair_product(t, kind, q, first):
        gather_wait(t, q, 1 - c)
        value = None
        for core in range(2):
            slot = 2 * chip_at(q) + core
            part = row_product(w_all[t, slot], x[kind // 2, :, columns_of(slot)])
            value = part if value is None else value + part
        if first:
            acc[kind] = value
        else:
            acc[kind] += value

    def by_rows(body):
        strip = 16

        def step(i, carry):
            body(pl.ds(pl.multiple_of(i * strip, strip), strip))
            return carry

        lax.fori_loop(0, height // strip, step, 0)

    def make_hidden(p):
        t = 3 * p + DOWN

        def strip(r):
            gate = acc[GATE, r, :]
            sig = jax.nn.sigmoid(gate)
            act = gate * sig
            up = acc[UP, r, :]
            cots[t, r, :] = (act * up).astype(jnp.bfloat16)
            acc[UP, r, :] = up * sig * (1.0 + gate * (1.0 - sig))
            acc[GATE, r, :] = act

        by_rows(strip)

    def make_cots(p):
        t = 3 * p

        def strip(r):
            hidden_grad = acc[DOWN, r, :]
            cots[t + GATE, r, :] = (hidden_grad * acc[UP, r, :]).astype(jnp.bfloat16)
            cots[t + UP, r, :] = (hidden_grad * acc[GATE, r, :]).astype(jnp.bfloat16)

        by_rows(strip)

    def side_of(g):
        return lax.rem(g, 3) // 2

    def term(g, slot):
        return jnp.dot(
            cots[g], x[side_of(g), :, columns_of(slot)], preferred_element_type=jnp.float32
        )

    def sibling_copy(g, chip):
        return pltpu.make_async_remote_copy(
            src_ref=sib_out.at[g, chip], dst_ref=sib_in.at[g, chip],
            send_sem=sib_send.at[g, chip], recv_sem=sib_recv.at[g, chip],
            device_id={"fs": other}, device_id_type=MESH,
        )

    def line_copy(g, way, chip):
        return pltpu.make_async_remote_copy(
            src_ref=line_out.at[g, chip], dst_ref=line_in.at[g, way, chip],
            send_sem=line_send.at[g, chip], recv_sem=line_recv.at[g, way, chip],
            device_id={"fs": line_device(way)}, device_id_type=MESH,
        )

    def sibling_terms(g, order):
        values = [term(g, 2 * chip_at(q) + 1 - c).astype(jnp.bfloat16) for q in order]
        for q, value in zip(order, values):
            sib_out[g, chip_at(q)] = value
        for q in order:
            sibling_copy(g, chip_at(q)).start()

    def own_terms(g, order):
        values = [term(g, 2 * chip_at(q) + c) for q in order]
        for q, value in zip(order, values):
            own_term[g, chip_at(q)] = value

    def pair_sum(g, chip):
        sibling_copy(g, chip).wait_recv()
        return own_term[g, chip] + sib_in[g, chip].astype(jnp.float32)

    def send_sum(g, q, way, relay):
        chip = chip_at(q)
        value = pair_sum(g, chip)
        if relay:
            line_copy(g, way, chip).wait_recv()
            value = value + line_in[g, way, chip].astype(jnp.float32)
        line_out[g, chip] = value.astype(jnp.bfloat16)
        line_copy(g, way, chip).start()

    side_peer = tp + 1 - 2 * lax.rem(tp, 2)
    far_peer = lax.rem(tp + 2, n_tp)
    corner = lax.rem(side_peer + 2, n_tp)
    half = ig_out.shape[0] // 2

    def half_rows(s):
        return pl.ds(s * half, half)

    def input_copy(k, source):
        s = k % 2
        peers = (side_peer, far_peer) if k < 4 else (far_peer, side_peer)
        return pltpu.make_async_remote_copy(
            src_ref=source, dst_ref=ig_in.at[k], send_sem=ig_send.at[k], recv_sem=ig_recv.at[k],
            device_id={"tp": peers[s]}, device_id_type=MESH,
        )

    def corner_copy(s):
        return input_copy(s, ig_part.at[corner, half_rows(s), :])

    def direct_copy(s):
        return input_copy(2 + s, ig_part.at[(side_peer, far_peer)[s], half_rows(s), :])

    def relay_copy(s):
        return input_copy(4 + s, ig_mid.at[s])

    def input_relay():
        for s in range(2):
            corner_copy(s).wait_recv()
            own = ig_part[(far_peer, side_peer)[s], half_rows(s), :].astype(jnp.float32)
            ig_mid[s] = (own + ig_in[s].astype(jnp.float32)).astype(jnp.bfloat16)
            relay_copy(s).start()

    def turn_cots(p):
        for kind in (GATE, UP):
            cots_turned[2 * p + kind] = cots[3 * p + kind].T

    def input_value(peer, some_parts):
        value = None
        for p in some_parts:
            for kind in (GATE, UP):
                block = jnp.concatenate(
                    [w_all[3 * p + kind, peer * pieces + i] for i in range(pieces)], axis=1
                )
                part = jnp.dot(
                    cots_turned[2 * p + kind], block, preferred_element_type=jnp.float32
                )
                value = part if value is None else value + part
        return value

    def input_base(turn):
        def body(peer, carry):
            ig_acc[peer] = input_value(peer, range(parts - 1))
            return carry

        share = n_tp // 2
        lax.fori_loop(turn * share, (turn + 1) * share, body, 0)

    def input_last():
        def body(step, carry):
            peer = jnp.where(
                step == 0, corner, jnp.where(step == 1, side_peer, jnp.where(step == 2, far_peer, tp))
            )
            value = ig_acc[peer] + input_value(peer, (parts - 1,))
            ig_part[peer] = value.astype(jnp.bfloat16)

            @pl.when(step == 0)
            def _():
                corner_copy(0).start()
                corner_copy(1).start()

            @pl.when(step == 1)
            def _():
                direct_copy(0).start()

            @pl.when(step == 2)
            def _():
                direct_copy(1).start()

            return carry

        lax.fori_loop(0, n_tp, body, 0)

    def end_gather(t, kind):
        gather_wait(t, 1, c)
        gather_copy(t, 1, SIBLING).start()
        pair_product(t, kind, 0, True)
        gather_wait(t, 2, c)
        gather_copy(t, 2, SIBLING).start()
        pair_product(t, kind, 1, False)
        gather_wait(t, 3, c)
        gather_copy(t, 3, SIBLING).start()
        pair_product(t, kind, 2, False)
        pair_product(t, kind, 3, False)

    def end_terms(low, high):
        def terms(g, carry):
            sibling_terms(g, (3, 2, 1, 0))
            return carry

        def own(g, carry):
            own_terms(g, (3, 2, 1, 0))
            return carry

        lax.fori_loop(low, high, terms, 0)
        lax.fori_loop(low, high, own, 0)

    def end_far(low, high):
        for q in (3, 2):
            def far(g, carry):
                send_sum(g, q, inward, False)
                return carry

            lax.fori_loop(low, high, far, 0)

    def end_near(low, high):
        def near(g, carry):
            send_sum(g, 1, inward, False)
            own_sum[g] = pair_sum(g, z)
            return carry

        lax.fori_loop(low, high, near, 0)

    def end_part(p, carry):
        first = 3 * p
        down = first + DOWN
        is_last = (p == parts - 1).astype(jnp.int32)

        def gate_or_up(kind, carry):
            @pl.when(p == parts - 1)
            def _():
                input_base(kind)

            end_gather(first + kind, kind)
            return carry

        lax.fori_loop(GATE, DOWN, gate_or_up, 0)
        make_hidden(p)
        end_terms(down, down + 1)
        end_far(down, down + 1)
        end_near(down + is_last, down + 1)

        end_gather(down, DOWN)
        make_cots(p)

        @pl.when(p == parts - 1)
        def _():
            turn_cots(p)
            input_last()

        end_terms(first, down)
        end_far(first, down)
        end_near(first, down + is_last)

        @pl.when(p < parts - 1)
        def _():
            turn_cots(p)
        return carry

    def relay_in(t):
        @pl.when(t < total)
        def _():
            gather_wait(t, 0, c)
            gather_copy(t, 0, inward).start()
            gather_copy(t, 0, SIBLING).start()

        @pl.when(t + OWN_IN < total)
        def _():
            gather_copy(t + OWN_IN, 1, inward).start()

    def relay_near(t):
        @pl.when(t < total)
        def _():
            gather_wait(t, 2, c)
            gather_copy(t, 2, outward).start()
            gather_copy(t, 2, SIBLING).start()

    def relay_far(t):
        @pl.when(t < total)
        def _():
            gather_wait(t, 3, c)
            gather_copy(t, 3, outward).start()
            gather_copy(t, 3, SIBLING).start()

        @pl.when(t + OWN_OUT < total)
        def _():
            gather_copy(t + OWN_OUT, 1, outward).start()

    def middle_gather(t, kind):
        relay_in(t + RELAY_IN)
        pair_product(t, kind, 1, True)
        relay_near(t + RELAY_OUT)
        pair_product(t, kind, 0, False)
        relay_far(t + RELAY_OUT)
        pair_product(t, kind, 2, False)
        pair_product(t, kind, 3, False)

    def in_turn(i):
        return 3 * (i // 3) + lax.rem(i + 2, 3)

    def final(r, carry):
        g = in_turn(r)
        line_copy(g, outward, z).wait_recv()
        own_sum[g] += line_in[g, outward, z].astype(jnp.float32)
        return carry

    def middle_final(r, carry):
        g = in_turn(r)
        for way in (inward, outward):
            line_copy(g, way, z).wait_recv()
        own_sum[g] += (
            line_in[g, inward, z].astype(jnp.float32) + line_in[g, outward, z].astype(jnp.float32)
        )
        return carry

    def middle_reduce(r):
        @pl.when(jnp.logical_and(r >= -1, r < total - 1))
        def _():
            g = in_turn(r + 1)
            sibling_terms(g, (3, 2, 0, 1))
            own_terms(g, (3, 2, 0, 1))

        @pl.when(jnp.logical_and(r >= 0, r < total))
        def _():
            send_sum(in_turn(r), 3, inward, True)

        @pl.when(jnp.logical_and(r >= LAG_OUT, r < total + LAG_OUT))
        def _():
            send_sum(in_turn(r - LAG_OUT), 0, outward, True)

        @pl.when(jnp.logical_and(r >= LAG_NEAR, r < total + LAG_NEAR))
        def _():
            g = in_turn(r - LAG_NEAR)
            send_sum(g, 2, inward, True)
            own_sum[g] = pair_sum(g, z)

        @pl.when(r >= LAG_FINAL)
        def _():
            middle_final(r - LAG_FINAL, 0)

    def middle_part(p, carry):
        for kind in (GATE, UP, DOWN):
            t = 3 * p + kind
            middle_gather(t, kind)
            if kind == UP:
                make_hidden(p)
            if kind == DOWN:
                make_cots(p)
            middle_reduce(t - LAG)
        turn_cots(p)
        return carry

    def middle_rest(r, carry):
        middle_reduce(r)
        turn = r - (total - LAG)

        @pl.when(turn < 2)
        def _():
            input_base(turn)

        @pl.when(turn == 2)
        def _():
            input_last()

        @pl.when(turn == INPUT_TURN)
        def _():
            input_relay()

        return carry

    for t in range(total):
        loads[t].wait()
        gather_copy(t, jnp.where(is_end, 0, 1), SIBLING).start()

        @pl.when(is_end)
        def _():
            gather_copy(t, 0, inward).start()

        if t < OWN_OUT:
            @pl.when(jnp.logical_not(is_end))
            def _():
                gather_copy(t, 1, outward).start()

        if t < OWN_IN:
            @pl.when(jnp.logical_not(is_end))
            def _():
                gather_copy(t, 1, inward).start()

    loads[total].wait()
    loads[total + 1].wait()

    @pl.when(is_end)
    def _():
        lax.fori_loop(0, parts, end_part, 0)
        input_relay()
        lax.fori_loop(0, total, final, 0)

    @pl.when(jnp.logical_not(is_end))
    def _():
        for t in range(RELAY_IN):
            relay_in(t)
        for t in range(RELAY_OUT):
            relay_near(t)
            relay_far(t)
        lax.fori_loop(0, parts, middle_part, 0)
        lax.fori_loop(total - LAG, total + LAG_OUT, middle_rest, 0)
        lax.fori_loop(total + LAG_OUT - LAG_FINAL, total, middle_final, 0)

    for s in range(2):
        direct_copy(s).wait_recv()
        relay_copy(s).wait_recv()
        value = ig_part[tp, half_rows(s), :].astype(jnp.float32)
        for k in (2 + s, 4 + s):
            value = value + ig_in[k].astype(jnp.float32)
        ig_out[half_rows(s), :] = value.astype(ig_out.dtype)

    def drain(g, carry):
        for chip in range(nz):
            gather_copy(g, chip, SIBLING).wait_send()
            sibling_copy(g, chip).wait_send()

            @pl.when(chip != z)
            def _():
                way = jnp.where(chip > z, RIGHT, LEFT)
                line_copy(g, way, chip).wait_send()

            @pl.when(jnp.logical_and(has_right, chip <= z))
            def _():
                absolute_copy(g, chip, RIGHT).wait_send()

            @pl.when(jnp.logical_and(has_left, chip >= z))
            def _():
                absolute_copy(g, chip, LEFT).wait_send()

        return carry

    def absolute_copy(t, chip, way):
        slot = 2 * chip + c
        return pltpu.make_async_remote_copy(
            src_ref=w_all.at[t, slot], dst_ref=w_all.at[t, slot],
            send_sem=ag_send.at[t, way, chip], recv_sem=ag_recv.at[t, slot],
            device_id={"fs": line_device(way)}, device_id_type=MESH,
        )

    lax.fori_loop(0, total, drain, 0)
    for s in range(2):
        for copy in (corner_copy, direct_copy, relay_copy):
            copy(s).wait_send()


def fused_shards(tokens, cotangent, gate_weight, up_weight, down_weight):
    n, n_tp = lax.axis_size("fs"), lax.axis_size("tp")
    nz = n // 2
    count, width = tokens.shape
    rows, hidden = gate_weight.shape
    height = hidden // PARTS
    pieces = 3 * PARTS
    share = width // n_tp
    bf16, f32 = jnp.bfloat16, jnp.float32
    dma = pltpu.SemaphoreType.DMA
    input_grad, sums = pl.pallas_call(
        functools.partial(kernel, n, n_tp, PARTS),
        out_shape=(pltpu.VMEM((count, share), bf16), pltpu.VMEM((pieces, height, rows), f32)),
        in_specs=[pl.BlockSpec(memory_space=pl.ANY)] * 5,
        out_specs=(pl.BlockSpec(memory_space=pltpu.VMEM),) * 2,
        scratch_shapes=[
            pltpu.VMEM((2, count, width), bf16),
            pltpu.VMEM((pieces, n, height, rows), bf16),
            pltpu.VMEM((3, height, count), f32),
            pltpu.VMEM((pieces, height, count), bf16),
            pltpu.VMEM((2 * PARTS, count, height), bf16),
            pltpu.VMEM((pieces, nz, height, rows), f32),
            pltpu.VMEM((pieces, nz, height, rows), bf16),
            pltpu.VMEM((pieces, nz, height, rows), bf16),
            pltpu.VMEM((pieces, nz, height, rows), bf16),
            pltpu.VMEM((pieces, 2, nz, height, rows), bf16),
            pltpu.VMEM((n_tp, count, share), f32),
            pltpu.VMEM((n_tp, count, share), bf16),
            pltpu.VMEM((6, count // 2, share), bf16),
            pltpu.VMEM((2, count // 2, share), bf16),
            dma((pieces + 2,)),
            dma((pieces, 3, nz)),
            dma((pieces, n)),
            dma((pieces, nz)),
            dma((pieces, nz)),
            dma((pieces, nz)),
            dma((pieces, 2, nz)),
            dma((6,)),
            dma((6,)),
        ],
        compiler_params=pltpu.CompilerParams(
            collective_id=0, has_side_effects=True, vmem_limit_bytes=VMEM_BYTES
        ),
    )(tokens, cotangent, gate_weight.T, up_weight.T, down_weight.T)
    input_grad, gate_grad, up_grad, down_grad = pl.pallas_call(
        functools.partial(deliver, PARTS),
        out_shape=(
            jax.ShapeDtypeStruct((count, share), bf16),
        ) + (jax.ShapeDtypeStruct((hidden, rows), f32),) * 3,
        in_specs=[pl.BlockSpec(memory_space=pltpu.VMEM)] * 2,
        out_specs=(pl.BlockSpec(memory_space=pl.ANY),) * 4,
        scratch_shapes=[dma((pieces + 1,))],
        compiler_params=pltpu.CompilerParams(vmem_limit_bytes=DELIVER_BYTES),
    )(*(pltpu.with_memory_space_constraint(v, pltpu.VMEM) for v in (input_grad, sums)))
    return input_grad, gate_grad.T, up_grad.T, down_grad.T


def deliver(parts, ig, sums, ig_out, gate_out, up_out, down_out, sem):
    height = sums.shape[1]
    copies = [pltpu.make_async_copy(ig, ig_out, sem.at[3 * parts])]
    for g in range(3 * parts):
        out = (gate_out, up_out, down_out)[g % 3]
        piece = pl.ds((g // 3) * height, height)
        copies.append(pltpu.make_async_copy(sums.at[g], out.at[piece, :], sem.at[g]))
    for copy in copies:
        copy.start()
    for copy in copies:
        copy.wait()


def shards(tokens, cotangent, gate_weight, up_weight, down_weight):
    n, n_tp = lax.axis_size("fs"), lax.axis_size("tp")
    rows = gate_weight.shape[0]
    share = tokens.shape[1] // n_tp
    if n == 2 * CHIPS and n_tp == 4 and rows % 128 == 0 and share % rows == 0 and (
        gate_weight.shape[1] % (16 * PARTS) == 0
    ):
        return fused_shards(tokens, cotangent, gate_weight, up_weight, down_weight)
    return plain_shards(tokens, cotangent, gate_weight, up_weight, down_weight)


def solution(mesh):
    in_specs = (P("fs", None), P("fs", None), P("fs", "tp"), P("fs", "tp"), P("fs", "tp"))
    out_specs = (P("fs", "tp"), P("fs", "tp"), P("fs", "tp"), P("fs", "tp"))
    return jax.shard_map(shards, mesh=mesh, in_specs=in_specs, out_specs=out_specs, check_vma=False)
```

```python
import functools

import jax
import jax.numpy as jnp
from jax import lax
from jax.experimental import pallas as pl
from jax.experimental.pallas import tpu as pltpu
from jax.sharding import PartitionSpec as P


def row_product(left, right):
    return lax.dot_general(
        left, right, (((1,), (1,)), ((), ())), preferred_element_type=jnp.float32
    )


def token_product(left, right):
    return lax.dot_general(
        left, right, (((0,), (0,)), ((), ())), preferred_element_type=jnp.float32
    )


def owner_sum(received, groups):
    return received.reshape(groups, received.shape[0] // groups, received.shape[1]).sum(axis=0)


def plain_shards(tokens, cotangent, gate_weight, up_weight, down_weight):
    groups = lax.axis_size("fs")
    whole_gate, whole_up, whole_down = (
        lax.all_gather(gate_weight, "fs", axis=0, tiled=True),
        lax.all_gather(up_weight, "fs", axis=0, tiled=True),
        lax.all_gather(down_weight, "fs", axis=0, tiled=True),
    )
    gate = jnp.dot(tokens, whole_gate, preferred_element_type=jnp.float32)
    up = jnp.dot(tokens, whole_up, preferred_element_type=jnp.float32)
    hidden_grad = jnp.dot(cotangent, whole_down, preferred_element_type=jnp.float32)
    sig = jax.nn.sigmoid(gate)
    act = gate * sig
    hidden = (act * up).astype(jnp.bfloat16)
    gate_cot = (hidden_grad * up * sig * (1.0 + gate * (1.0 - sig))).astype(jnp.bfloat16)
    up_cot = (hidden_grad * act).astype(jnp.bfloat16)
    partial_value = row_product(gate_cot, whole_gate) + row_product(up_cot, whole_up)
    input_grad = lax.psum_scatter(
        partial_value.astype(jnp.bfloat16), "tp", scatter_dimension=1, tiled=True
    )
    gate_term = token_product(tokens, gate_cot)
    gate_grad = owner_sum(
        lax.all_to_all(
            gate_term.astype(jnp.bfloat16), "fs", split_axis=0, concat_axis=0, tiled=True
        ).astype(gate_term.dtype),
        groups,
    )
    up_term = token_product(tokens, up_cot)
    up_grad = owner_sum(
        lax.all_to_all(
            up_term.astype(jnp.bfloat16), "fs", split_axis=0, concat_axis=0, tiled=True
        ).astype(up_term.dtype),
        groups,
    )
    down_term = token_product(cotangent, hidden)
    down_grad = owner_sum(
        lax.all_to_all(
            down_term.astype(jnp.bfloat16), "fs", split_axis=0, concat_axis=0, tiled=True
        ).astype(down_term.dtype),
        groups,
    )
    return (input_grad, gate_grad, up_grad, down_grad)


MESH = pl.DeviceIdType.MESH
PARTS = 4
CHIPS = 4
LAG = 7
VMEM_BYTES = 60 * 1024 * 1024
DELIVER_BYTES = 1024 * 1024
LAG_OUT, LAG_NEAR, LAG_FINAL = 3, 1, 5
INPUT_TURN = 5
OWN_IN, OWN_OUT = 1, 1
FIRST_IN, FIRST_OUT = 2, 3
RELAY_IN, RELAY_OUT = 2, 1
GATE, UP, DOWN = 0, 1, 2
RIGHT, LEFT, SIBLING = 0, 1, 2


def kernel(
    n, n_tp, parts, tok, cot, gw, uw, dw, ig_out, own_sum,
    x, w_all, acc, cots, cots_turned, own_term, sib_out, sib_in, line_out, line_in, ig_acc, ig_part, ig_in, ig_mid,
    local_sem, ag_send, ag_recv, sib_send, sib_recv, line_send, line_recv, ig_send, ig_recv,
):
    me, tp = lax.axis_index("fs"), lax.axis_index("tp")
    z, c = me // 2, me % 2
    nz = n // 2
    total = 3 * parts
    other = 2 * z + 1 - c
    rows = gw.shape[1]
    height = gw.shape[0] // parts
    own_columns = ig_out.shape[1]
    pieces = own_columns // rows
    mirrored = z >= nz // 2
    is_end = jnp.logical_or(z == 0, z == nz - 1)
    inward = jnp.where(mirrored, LEFT, RIGHT)
    outward = jnp.where(mirrored, RIGHT, LEFT)

    def chip_at(q):
        return jnp.where(mirrored, nz - 1 - q, q)

    def weight_load(t):
        piece = pl.ds((t // 3) * height, height)
        return pltpu.make_async_copy(
            (gw, uw, dw)[t % 3].at[piece, :], w_all.at[t, me], local_sem.at[t]
        )

    loads = [weight_load(t) for t in range(total)]
    loads += [
        pltpu.make_async_copy(tok, x.at[0], local_sem.at[total]),
        pltpu.make_async_copy(cot, x.at[1], local_sem.at[total + 1]),
    ]
    for load in loads[:total]:
        load.start()

    has_left, has_right = z > 0, z < nz - 1
    barrier = pltpu.get_barrier_semaphore()
    pl.semaphore_signal(barrier, inc=1, device_id={"fs": other}, device_id_type=MESH)
    for step in range(1, n_tp):
        pl.semaphore_signal(
            barrier, inc=1, device_id={"tp": lax.rem(tp + step, n_tp)}, device_id_type=MESH
        )

    @pl.when(has_right)
    def _():
        pl.semaphore_signal(barrier, inc=1, device_id={"fs": me + 2}, device_id_type=MESH)

    @pl.when(has_left)
    def _():
        pl.semaphore_signal(barrier, inc=1, device_id={"fs": me - 2}, device_id_type=MESH)

    pl.semaphore_wait(barrier, n_tp + has_left.astype(jnp.int32) + has_right.astype(jnp.int32))

    def line_device(way):
        return me + 2 - 4 * way

    def gather_copy(t, q, way):
        chip = chip_at(q)
        slot = 2 * chip + c
        device = other if way is SIBLING else line_device(way)
        return pltpu.make_async_remote_copy(
            src_ref=w_all.at[t, slot], dst_ref=w_all.at[t, slot],
            send_sem=ag_send.at[t, way, chip], recv_sem=ag_recv.at[t, slot],
            device_id={"fs": device}, device_id_type=MESH,
        )

    def gather_wait(t, q, core):
        slot = 2 * chip_at(q) + core
        pltpu.make_async_remote_copy(
            src_ref=w_all.at[t, slot], dst_ref=w_all.at[t, slot],
            send_sem=ag_send.at[t, SIBLING, 0], recv_sem=ag_recv.at[t, slot],
            device_id={"fs": other}, device_id_type=MESH,
        ).wait_recv()

    def columns_of(slot):
        return pl.ds(pl.multiple_of(slot * rows, rows), rows)

    def pair_product(t, kind, q, first):
        gather_wait(t, q, 1 - c)
        value = None
        for core in range(2):
            slot = 2 * chip_at(q) + core
            part = row_product(w_all[t, slot], x[kind // 2, :, columns_of(slot)])
            value = part if value is None else value + part
        if first:
            acc[kind] = value
        else:
            acc[kind] += value

    def by_rows(body):
        strip = 16

        def step(i, carry):
            body(pl.ds(pl.multiple_of(i * strip, strip), strip))
            return carry

        lax.fori_loop(0, height // strip, step, 0)

    def make_hidden(p):
        t = 3 * p + DOWN

        def strip(r):
            gate = acc[GATE, r, :]
            sig = jax.nn.sigmoid(gate)
            act = gate * sig
            up = acc[UP, r, :]
            cots[t, r, :] = (act * up).astype(jnp.bfloat16)
            acc[UP, r, :] = up * sig * (1.0 + gate * (1.0 - sig))
            acc[GATE, r, :] = act

        by_rows(strip)

    def make_cots(p):
        t = 3 * p

        def strip(r):
            hidden_grad = acc[DOWN, r, :]
            cots[t + GATE, r, :] = (hidden_grad * acc[UP, r, :]).astype(jnp.bfloat16)
            cots[t + UP, r, :] = (hidden_grad * acc[GATE, r, :]).astype(jnp.bfloat16)

        by_rows(strip)

    def side_of(g):
        return lax.rem(g, 3) // 2

    def term(g, slot):
        return jnp.dot(
            cots[g], x[side_of(g), :, columns_of(slot)], preferred_element_type=jnp.float32
        )

    def sibling_copy(g, chip):
        return pltpu.make_async_remote_copy(
            src_ref=sib_out.at[g, chip], dst_ref=sib_in.at[g, chip],
            send_sem=sib_send.at[g, chip], recv_sem=sib_recv.at[g, chip],
            device_id={"fs": other}, device_id_type=MESH,
        )

    def line_copy(g, way, chip):
        return pltpu.make_async_remote_copy(
            src_ref=line_out.at[g, chip], dst_ref=line_in.at[g, way, chip],
            send_sem=line_send.at[g, chip], recv_sem=line_recv.at[g, way, chip],
            device_id={"fs": line_device(way)}, device_id_type=MESH,
        )

    def sibling_terms(g, order):
        values = [term(g, 2 * chip_at(q) + 1 - c).astype(jnp.bfloat16) for q in order]
        for q, value in zip(order, values):
            sib_out[g, chip_at(q)] = value
        for q in order:
            sibling_copy(g, chip_at(q)).start()

    def own_terms(g, order):
        values = [term(g, 2 * chip_at(q) + c) for q in order]
        for q, value in zip(order, values):
            own_term[g, chip_at(q)] = value

    def pair_sum(g, chip):
        sibling_copy(g, chip).wait_recv()
        return own_term[g, chip] + sib_in[g, chip].astype(jnp.float32)

    def send_sum(g, q, way, relay):
        chip = chip_at(q)
        value = pair_sum(g, chip)
        if relay:
            line_copy(g, way, chip).wait_recv()
            value = value + line_in[g, way, chip].astype(jnp.float32)
        line_out[g, chip] = value.astype(jnp.bfloat16)
        line_copy(g, way, chip).start()

    side_peer = tp + 1 - 2 * lax.rem(tp, 2)
    far_peer = lax.rem(tp + 2, n_tp)
    corner = lax.rem(side_peer + 2, n_tp)
    half = ig_out.shape[0] // 2

    def half_rows(s):
        return pl.ds(s * half, half)

    def input_copy(k, source):
        s = k % 2
        peers = (side_peer, far_peer) if k < 4 else (far_peer, side_peer)
        return pltpu.make_async_remote_copy(
            src_ref=source, dst_ref=ig_in.at[k], send_sem=ig_send.at[k], recv_sem=ig_recv.at[k],
            device_id={"tp": peers[s]}, device_id_type=MESH,
        )

    def corner_copy(s):
        return input_copy(s, ig_part.at[corner, half_rows(s), :])

    def direct_copy(s):
        return input_copy(2 + s, ig_part.at[(side_peer, far_peer)[s], half_rows(s), :])

    def relay_copy(s):
        return input_copy(4 + s, ig_mid.at[s])

    def input_relay():
        for s in range(2):
            corner_copy(s).wait_recv()
            own = ig_part[(far_peer, side_peer)[s], half_rows(s), :].astype(jnp.float32)
            ig_mid[s] = (own + ig_in[s].astype(jnp.float32)).astype(jnp.bfloat16)
            relay_copy(s).start()

    def turn_cots(p):
        for kind in (GATE, UP):
            cots_turned[2 * p + kind] = cots[3 * p + kind].T

    def input_value(peer, some_parts):
        value = None
        for p in some_parts:
            for kind in (GATE, UP):
                block = jnp.concatenate(
                    [w_all[3 * p + kind, peer * pieces + i] for i in range(pieces)], axis=1
                )
                part = jnp.dot(
                    cots_turned[2 * p + kind], block, preferred_element_type=jnp.float32
                )
                value = part if value is None else value + part
        return value

    def input_base(turn):
        def body(peer, carry):
            ig_acc[peer] = input_value(peer, range(parts - 1))
            return carry

        share = n_tp // 2
        lax.fori_loop(turn * share, (turn + 1) * share, body, 0)

    def input_last():
        def body(step, carry):
            peer = jnp.where(
                step == 0, corner, jnp.where(step == 1, side_peer, jnp.where(step == 2, far_peer, tp))
            )
            value = ig_acc[peer] + input_value(peer, (parts - 1,))
            ig_part[peer] = value.astype(jnp.bfloat16)

            @pl.when(step == 0)
            def _():
                corner_copy(0).start()
                corner_copy(1).start()

            @pl.when(step == 1)
            def _():
                direct_copy(0).start()

            @pl.when(step == 2)
            def _():
                direct_copy(1).start()

            return carry

        lax.fori_loop(0, n_tp, body, 0)

    def drain_early(g, carry):
        for q in range(nz):
            gather_copy(g, q, SIBLING).wait_send()
            sibling_copy(g, chip_at(q)).wait_send()
        return carry

    def end_drain(g, carry):
        gather_copy(g, 0, inward).wait_send()
        return drain_early(g, carry)

    def middle_drain(g, carry):
        for q in (1, 2, 3):
            gather_copy(g, q, outward).wait_send()
        for q in (0, 1):
            gather_copy(g, q, inward).wait_send()
        return drain_early(g, carry)

    def end_gather(t, kind):
        gather_wait(t, 1, c)
        gather_copy(t, 1, SIBLING).start()
        pair_product(t, kind, 0, True)
        gather_wait(t, 2, c)
        gather_copy(t, 2, SIBLING).start()
        pair_product(t, kind, 1, False)
        gather_wait(t, 3, c)
        gather_copy(t, 3, SIBLING).start()
        pair_product(t, kind, 2, False)
        pair_product(t, kind, 3, False)

    def end_terms(low, high):
        def terms(g, carry):
            sibling_terms(g, (3, 2, 1, 0))
            return carry

        def own(g, carry):
            own_terms(g, (3, 2, 1, 0))
            return carry

        lax.fori_loop(low, high, terms, 0)
        lax.fori_loop(low, high, own, 0)

    def end_far(low, high):
        for q in (3, 2):
            def far(g, carry):
                send_sum(g, q, inward, False)
                return carry

            lax.fori_loop(low, high, far, 0)

    def end_near(low, high):
        def near(g, carry):
            send_sum(g, 1, inward, False)
            own_sum[g] = pair_sum(g, z)
            return carry

        lax.fori_loop(low, high, near, 0)

    def end_part(p, carry):
        first = 3 * p
        down = first + DOWN
        is_last = (p == parts - 1).astype(jnp.int32)

        def gate_or_up(kind, carry):
            @pl.when(p == parts - 1)
            def _():
                input_base(kind)

            end_gather(first + kind, kind)
            return carry

        lax.fori_loop(GATE, DOWN, gate_or_up, 0)
        make_hidden(p)
        end_terms(down, down + 1)
        end_far(down, down + 1)
        end_near(down + is_last, down + 1)

        end_gather(down, DOWN)
        make_cots(p)

        @pl.when(p == parts - 1)
        def _():
            turn_cots(p)
            input_last()

        end_terms(first, down)
        end_far(first, down)
        end_near(first, down + is_last)

        @pl.when(p < parts - 1)
        def _():
            turn_cots(p)
        return carry

    def relay_in(t):
        @pl.when(t < total)
        def _():
            gather_wait(t, 0, c)
            gather_copy(t, 0, inward).start()
            gather_copy(t, 0, SIBLING).start()

        @pl.when(jnp.logical_and(t + OWN_IN >= FIRST_IN, t + OWN_IN < total))
        def _():
            gather_copy(t + OWN_IN, 1, inward).start()

    def relay_near(t):
        @pl.when(t < total)
        def _():
            gather_wait(t, 2, c)
            gather_copy(t, 2, outward).start()
            gather_copy(t, 2, SIBLING).start()

    def relay_far(t):
        @pl.when(t < total)
        def _():
            gather_wait(t, 3, c)
            gather_copy(t, 3, outward).start()
            gather_copy(t, 3, SIBLING).start()

        @pl.when(jnp.logical_and(t + OWN_OUT >= FIRST_OUT, t + OWN_OUT < total))
        def _():
            gather_copy(t + OWN_OUT, 1, outward).start()

    def middle_gather(t, kind):
        relay_in(t + RELAY_IN)
        pair_product(t, kind, 1, True)
        relay_near(t + RELAY_OUT)
        pair_product(t, kind, 0, False)
        relay_far(t + RELAY_OUT)
        pair_product(t, kind, 2, False)
        pair_product(t, kind, 3, False)

    def in_turn(i):
        return 3 * (i // 3) + lax.rem(i + 2, 3)

    def final(r, carry):
        g = in_turn(r)
        line_copy(g, outward, z).wait_recv()
        own_sum[g] += line_in[g, outward, z].astype(jnp.float32)
        return carry

    def middle_final(r, carry):
        g = in_turn(r)
        for way in (inward, outward):
            line_copy(g, way, z).wait_recv()
        own_sum[g] += (
            line_in[g, inward, z].astype(jnp.float32) + line_in[g, outward, z].astype(jnp.float32)
        )
        return carry

    def middle_reduce(r):
        @pl.when(jnp.logical_and(r >= -1, r < total - 1))
        def _():
            g = in_turn(r + 1)
            sibling_terms(g, (3, 2, 0, 1))
            own_terms(g, (3, 2, 0, 1))

        @pl.when(jnp.logical_and(r >= 0, r < total))
        def _():
            send_sum(in_turn(r), 3, inward, True)

        @pl.when(jnp.logical_and(r >= LAG_OUT, r < total + LAG_OUT))
        def _():
            send_sum(in_turn(r - LAG_OUT), 0, outward, True)

        @pl.when(jnp.logical_and(r >= LAG_NEAR, r < total + LAG_NEAR))
        def _():
            g = in_turn(r - LAG_NEAR)
            send_sum(g, 2, inward, True)
            own_sum[g] = pair_sum(g, z)

        @pl.when(r >= LAG_FINAL)
        def _():
            middle_final(r - LAG_FINAL, 0)

    def middle_part(p, carry):
        for kind in (GATE, UP, DOWN):
            t = 3 * p + kind
            middle_gather(t, kind)
            if kind == UP:
                make_hidden(p)
            if kind == DOWN:
                make_cots(p)
            middle_reduce(t - LAG)
        turn_cots(p)
        return carry

    def middle_rest(r, carry):
        middle_reduce(r)
        turn = r - (total - LAG)

        @pl.when(turn < 2)
        def _():
            input_base(turn)

        @pl.when(turn == 2)
        def _():
            input_last()

        @pl.when(jnp.logical_and(turn > 2, turn < 8))
        def _():
            lax.fori_loop((turn - 3) * 2, (turn - 2) * 2, middle_drain, 0)

        @pl.when(turn == INPUT_TURN)
        def _():
            input_relay()

        return carry

    for t in range(total):
        if t == FIRST_OUT:
            for load in loads[total:]:
                load.start()
        loads[t].wait()
        gather_copy(t, jnp.where(is_end, 0, 1), SIBLING).start()

        @pl.when(is_end)
        def _():
            gather_copy(t, 0, inward).start()

        if t < FIRST_OUT:
            @pl.when(jnp.logical_not(is_end))
            def _():
                gather_copy(t, 1, outward).start()

        if t < FIRST_IN:
            @pl.when(jnp.logical_not(is_end))
            def _():
                gather_copy(t, 1, inward).start()

    for load in loads[total:]:
        load.wait()

    @pl.when(is_end)
    def _():
        lax.fori_loop(0, parts, end_part, 0)
        input_relay()
        lax.fori_loop(0, total, end_drain, 0)
        lax.fori_loop(0, total, final, 0)

    @pl.when(jnp.logical_not(is_end))
    def _():
        for t in range(RELAY_IN):
            relay_in(t)
        for t in range(RELAY_OUT):
            relay_near(t)
            relay_far(t)
        lax.fori_loop(0, parts, middle_part, 0)
        lax.fori_loop(total - LAG, total + LAG_OUT, middle_rest, 0)
        lax.fori_loop(total - 2, total, middle_drain, 0)
        lax.fori_loop(total + LAG_OUT - LAG_FINAL, total, middle_final, 0)

    for s in range(2):
        direct_copy(s).wait_recv()
        relay_copy(s).wait_recv()
        value = ig_part[tp, half_rows(s), :].astype(jnp.float32)
        for k in (2 + s, 4 + s):
            value = value + ig_in[k].astype(jnp.float32)
        ig_out[half_rows(s), :] = value.astype(ig_out.dtype)

    def drain_lines(r, carry):
        g = in_turn(r)
        for q in range(nz):
            chip = chip_at(q)

            @pl.when(chip != z)
            def _():
                way = jnp.where(chip > z, RIGHT, LEFT)
                line_copy(g, way, chip).wait_send()

        return carry

    lax.fori_loop(0, total, drain_lines, 0)
    for s in range(2):
        for copy in (corner_copy, direct_copy, relay_copy):
            copy(s).wait_send()


def fused_shards(tokens, cotangent, gate_weight, up_weight, down_weight):
    n, n_tp = lax.axis_size("fs"), lax.axis_size("tp")
    nz = n // 2
    count, width = tokens.shape
    rows, hidden = gate_weight.shape
    height = hidden // PARTS
    pieces = 3 * PARTS
    share = width // n_tp
    bf16, f32 = jnp.bfloat16, jnp.float32
    dma = pltpu.SemaphoreType.DMA
    input_grad, sums = pl.pallas_call(
        functools.partial(kernel, n, n_tp, PARTS),
        out_shape=(pltpu.VMEM((count, share), bf16), pltpu.VMEM((pieces, height, rows), f32)),
        in_specs=[pl.BlockSpec(memory_space=pl.ANY)] * 5,
        out_specs=(pl.BlockSpec(memory_space=pltpu.VMEM),) * 2,
        scratch_shapes=[
            pltpu.VMEM((2, count, width), bf16),
            pltpu.VMEM((pieces, n, height, rows), bf16),
            pltpu.VMEM((3, height, count), f32),
            pltpu.VMEM((pieces, height, count), bf16),
            pltpu.VMEM((2 * PARTS, count, height), bf16),
            pltpu.VMEM((pieces, nz, height, rows), f32),
            pltpu.VMEM((pieces, nz, height, rows), bf16),
            pltpu.VMEM((pieces, nz, height, rows), bf16),
            pltpu.VMEM((pieces, nz, height, rows), bf16),
            pltpu.VMEM((pieces, 2, nz, height, rows), bf16),
            pltpu.VMEM((n_tp, count, share), f32),
            pltpu.VMEM((n_tp, count, share), bf16),
            pltpu.VMEM((6, count // 2, share), bf16),
            pltpu.VMEM((2, count // 2, share), bf16),
            dma((pieces + 2,)),
            dma((pieces, 3, nz)),
            dma((pieces, n)),
            dma((pieces, nz)),
            dma((pieces, nz)),
            dma((pieces, nz)),
            dma((pieces, 2, nz)),
            dma((6,)),
            dma((6,)),
        ],
        compiler_params=pltpu.CompilerParams(
            collective_id=0, has_side_effects=True, vmem_limit_bytes=VMEM_BYTES
        ),
    )(tokens, cotangent, gate_weight.T, up_weight.T, down_weight.T)
    input_grad, gate_grad, up_grad, down_grad = pl.pallas_call(
        functools.partial(deliver, PARTS),
        out_shape=(
            jax.ShapeDtypeStruct((count, share), bf16),
        ) + (jax.ShapeDtypeStruct((hidden, rows), f32),) * 3,
        in_specs=[pl.BlockSpec(memory_space=pltpu.VMEM)] * 2,
        out_specs=(pl.BlockSpec(memory_space=pl.ANY),) * 4,
        scratch_shapes=[dma((pieces + 1,))],
        compiler_params=pltpu.CompilerParams(vmem_limit_bytes=DELIVER_BYTES),
    )(*(pltpu.with_memory_space_constraint(v, pltpu.VMEM) for v in (input_grad, sums)))
    return input_grad, gate_grad.T, up_grad.T, down_grad.T


def deliver(parts, ig, sums, ig_out, gate_out, up_out, down_out, sem):
    height = sums.shape[1]
    copies = [pltpu.make_async_copy(ig, ig_out, sem.at[3 * parts])]
    for g in range(3 * parts):
        out = (gate_out, up_out, down_out)[g % 3]
        piece = pl.ds((g // 3) * height, height)
        copies.append(pltpu.make_async_copy(sums.at[g], out.at[piece, :], sem.at[g]))
    for copy in copies:
        copy.start()
    for copy in copies:
        copy.wait()


def shards(tokens, cotangent, gate_weight, up_weight, down_weight):
    n, n_tp = lax.axis_size("fs"), lax.axis_size("tp")
    rows = gate_weight.shape[0]
    share = tokens.shape[1] // n_tp
    if n == 2 * CHIPS and n_tp == 4 and rows % 128 == 0 and share % rows == 0 and (
        gate_weight.shape[1] % (16 * PARTS) == 0
    ):
        return fused_shards(tokens, cotangent, gate_weight, up_weight, down_weight)
    return plain_shards(tokens, cotangent, gate_weight, up_weight, down_weight)


def solution(mesh):
    in_specs = (P("fs", None), P("fs", None), P("fs", "tp"), P("fs", "tp"), P("fs", "tp"))
    out_specs = (P("fs", "tp"), P("fs", "tp"), P("fs", "tp"), P("fs", "tp"))
    return jax.shard_map(shards, mesh=mesh, in_specs=in_specs, out_specs=out_specs, check_vma=False)
```

```python
import functools

import jax
import jax.numpy as jnp
from jax import lax
from jax.experimental import pallas as pl
from jax.experimental.pallas import tpu as pltpu
from jax.sharding import PartitionSpec as P


def row_product(left, right):
    return lax.dot_general(
        left, right, (((1,), (1,)), ((), ())), preferred_element_type=jnp.float32
    )


def token_product(left, right):
    return lax.dot_general(
        left, right, (((0,), (0,)), ((), ())), preferred_element_type=jnp.float32
    )


def owner_sum(received, groups):
    return received.reshape(groups, received.shape[0] // groups, received.shape[1]).sum(axis=0)


def plain_shards(tokens, cotangent, gate_weight, up_weight, down_weight):
    groups = lax.axis_size("fs")
    whole_gate, whole_up, whole_down = (
        lax.all_gather(gate_weight, "fs", axis=0, tiled=True),
        lax.all_gather(up_weight, "fs", axis=0, tiled=True),
        lax.all_gather(down_weight, "fs", axis=0, tiled=True),
    )
    gate = jnp.dot(tokens, whole_gate, preferred_element_type=jnp.float32)
    up = jnp.dot(tokens, whole_up, preferred_element_type=jnp.float32)
    hidden_grad = jnp.dot(cotangent, whole_down, preferred_element_type=jnp.float32)
    sig = jax.nn.sigmoid(gate)
    act = gate * sig
    hidden = (act * up).astype(jnp.bfloat16)
    gate_cot = (hidden_grad * up * sig * (1.0 + gate * (1.0 - sig))).astype(jnp.bfloat16)
    up_cot = (hidden_grad * act).astype(jnp.bfloat16)
    partial_value = row_product(gate_cot, whole_gate) + row_product(up_cot, whole_up)
    input_grad = lax.psum_scatter(
        partial_value.astype(jnp.bfloat16), "tp", scatter_dimension=1, tiled=True
    )
    gate_term = token_product(tokens, gate_cot)
    gate_grad = owner_sum(
        lax.all_to_all(
            gate_term.astype(jnp.bfloat16), "fs", split_axis=0, concat_axis=0, tiled=True
        ).astype(gate_term.dtype),
        groups,
    )
    up_term = token_product(tokens, up_cot)
    up_grad = owner_sum(
        lax.all_to_all(
            up_term.astype(jnp.bfloat16), "fs", split_axis=0, concat_axis=0, tiled=True
        ).astype(up_term.dtype),
        groups,
    )
    down_term = token_product(cotangent, hidden)
    down_grad = owner_sum(
        lax.all_to_all(
            down_term.astype(jnp.bfloat16), "fs", split_axis=0, concat_axis=0, tiled=True
        ).astype(down_term.dtype),
        groups,
    )
    return (input_grad, gate_grad, up_grad, down_grad)


MESH = pl.DeviceIdType.MESH
PARTS = 4
CHIPS = 4
LAG = 7
VMEM_BYTES = 60 * 1024 * 1024
DELIVER_BYTES = 1024 * 1024
LAG_OUT, LAG_NEAR, LAG_FINAL = 3, 2, 5
INPUT_TURN = 5
OWN_IN, OWN_OUT = 1, 1
FIRST_IN, FIRST_OUT = 2, 3
RELAY_IN, RELAY_OUT = 2, 1
GATE, UP, DOWN = 0, 1, 2
RIGHT, LEFT, SIBLING = 0, 1, 2


def kernel(
    n, n_tp, parts, tok, cot, gw, uw, dw, ig_out, own_sum,
    x, w_all, acc, cots, cots_turned, own_term, sib_out, sib_in, line_out, line_in, ig_acc, ig_part, ig_in, ig_mid,
    local_sem, ag_send, ag_recv, sib_send, sib_recv, line_send, line_recv, ig_send, ig_recv,
):
    me, tp = lax.axis_index("fs"), lax.axis_index("tp")
    z, c = me // 2, me % 2
    nz = n // 2
    total = 3 * parts
    other = 2 * z + 1 - c
    rows = gw.shape[1]
    height = gw.shape[0] // parts
    own_columns = ig_out.shape[1]
    pieces = own_columns // rows
    mirrored = z >= nz // 2
    is_end = jnp.logical_or(z == 0, z == nz - 1)
    inward = jnp.where(mirrored, LEFT, RIGHT)
    outward = jnp.where(mirrored, RIGHT, LEFT)

    def chip_at(q):
        return jnp.where(mirrored, nz - 1 - q, q)

    def weight_load(t):
        piece = pl.ds((t // 3) * height, height)
        return pltpu.make_async_copy(
            (gw, uw, dw)[t % 3].at[piece, :], w_all.at[t, me], local_sem.at[t]
        )

    loads = [weight_load(t) for t in range(total)]
    loads += [
        pltpu.make_async_copy(tok, x.at[0], local_sem.at[total]),
        pltpu.make_async_copy(cot, x.at[1], local_sem.at[total + 1]),
    ]
    for load in loads[:total]:
        load.start()

    has_left, has_right = z > 0, z < nz - 1
    barrier = pltpu.get_barrier_semaphore()
    pl.semaphore_signal(barrier, inc=1, device_id={"fs": other}, device_id_type=MESH)
    for step in range(1, n_tp):
        pl.semaphore_signal(
            barrier, inc=1, device_id={"tp": lax.rem(tp + step, n_tp)}, device_id_type=MESH
        )

    @pl.when(has_right)
    def _():
        pl.semaphore_signal(barrier, inc=1, device_id={"fs": me + 2}, device_id_type=MESH)

    @pl.when(has_left)
    def _():
        pl.semaphore_signal(barrier, inc=1, device_id={"fs": me - 2}, device_id_type=MESH)

    pl.semaphore_wait(barrier, n_tp + has_left.astype(jnp.int32) + has_right.astype(jnp.int32))

    def line_device(way):
        return me + 2 - 4 * way

    def gather_copy(t, q, way):
        chip = chip_at(q)
        slot = 2 * chip + c
        device = other if way is SIBLING else line_device(way)
        return pltpu.make_async_remote_copy(
            src_ref=w_all.at[t, slot], dst_ref=w_all.at[t, slot],
            send_sem=ag_send.at[t, way, chip], recv_sem=ag_recv.at[t, slot],
            device_id={"fs": device}, device_id_type=MESH,
        )

    def gather_wait(t, q, core):
        slot = 2 * chip_at(q) + core
        pltpu.make_async_remote_copy(
            src_ref=w_all.at[t, slot], dst_ref=w_all.at[t, slot],
            send_sem=ag_send.at[t, SIBLING, 0], recv_sem=ag_recv.at[t, slot],
            device_id={"fs": other}, device_id_type=MESH,
        ).wait_recv()

    def columns_of(slot):
        return pl.ds(pl.multiple_of(slot * rows, rows), rows)

    def pair_product(t, kind, q, first):
        gather_wait(t, q, 1 - c)
        value = None
        for core in range(2):
            slot = 2 * chip_at(q) + core
            part = row_product(w_all[t, slot], x[kind // 2, :, columns_of(slot)])
            value = part if value is None else value + part
        if first:
            acc[kind] = value
        else:
            acc[kind] += value

    def by_rows(body):
        strip = 16

        def step(i, carry):
            body(pl.ds(pl.multiple_of(i * strip, strip), strip))
            return carry

        lax.fori_loop(0, height // strip, step, 0)

    def make_hidden(p):
        t = 3 * p + DOWN

        def strip(r):
            gate = acc[GATE, r, :]
            sig = jax.nn.sigmoid(gate)
            act = gate * sig
            up = acc[UP, r, :]
            cots[t, r, :] = (act * up).astype(jnp.bfloat16)
            acc[UP, r, :] = up * sig * (1.0 + gate * (1.0 - sig))
            acc[GATE, r, :] = act

        by_rows(strip)

    def make_cots(p):
        t = 3 * p

        def strip(r):
            hidden_grad = acc[DOWN, r, :]
            cots[t + GATE, r, :] = (hidden_grad * acc[UP, r, :]).astype(jnp.bfloat16)
            cots[t + UP, r, :] = (hidden_grad * acc[GATE, r, :]).astype(jnp.bfloat16)

        by_rows(strip)

    def side_of(g):
        return lax.rem(g, 3) // 2

    def term(g, slot):
        return jnp.dot(
            cots[g], x[side_of(g), :, columns_of(slot)], preferred_element_type=jnp.float32
        )

    def sibling_copy(g, chip):
        return pltpu.make_async_remote_copy(
            src_ref=sib_out.at[g, chip], dst_ref=sib_in.at[g, chip],
            send_sem=sib_send.at[g, chip], recv_sem=sib_recv.at[g, chip],
            device_id={"fs": other}, device_id_type=MESH,
        )

    def line_copy(g, way, chip):
        return pltpu.make_async_remote_copy(
            src_ref=line_out.at[g, chip], dst_ref=line_in.at[g, way, chip],
            send_sem=line_send.at[g, chip], recv_sem=line_recv.at[g, way, chip],
            device_id={"fs": line_device(way)}, device_id_type=MESH,
        )

    def sibling_terms(g, order):
        values = [term(g, 2 * chip_at(q) + 1 - c).astype(jnp.bfloat16) for q in order]
        for q, value in zip(order, values):
            sib_out[g, chip_at(q)] = value
        for q in order:
            sibling_copy(g, chip_at(q)).start()

    def own_terms(g, order):
        values = [term(g, 2 * chip_at(q) + c) for q in order]
        for q, value in zip(order, values):
            own_term[g, chip_at(q)] = value

    def pair_sum(g, chip):
        sibling_copy(g, chip).wait_recv()
        return own_term[g, chip] + sib_in[g, chip].astype(jnp.float32)

    def send_sum(g, q, way, relay):
        chip = chip_at(q)
        value = pair_sum(g, chip)
        if relay:
            line_copy(g, way, chip).wait_recv()
            value = value + line_in[g, way, chip].astype(jnp.float32)
        line_out[g, chip] = value.astype(jnp.bfloat16)
        line_copy(g, way, chip).start()

    side_peer = tp + 1 - 2 * lax.rem(tp, 2)
    far_peer = lax.rem(tp + 2, n_tp)
    corner = lax.rem(side_peer + 2, n_tp)
    half = ig_out.shape[0] // 2

    def half_rows(s):
        return pl.ds(s * half, half)

    def input_copy(k, source):
        s = k % 2
        peers = (side_peer, far_peer) if k < 4 else (far_peer, side_peer)
        return pltpu.make_async_remote_copy(
            src_ref=source, dst_ref=ig_in.at[k], send_sem=ig_send.at[k], recv_sem=ig_recv.at[k],
            device_id={"tp": peers[s]}, device_id_type=MESH,
        )

    def corner_copy(s):
        return input_copy(s, ig_part.at[corner, half_rows(s), :])

    def direct_copy(s):
        return input_copy(2 + s, ig_part.at[(side_peer, far_peer)[s], half_rows(s), :])

    def relay_copy(s):
        return input_copy(4 + s, ig_mid.at[s])

    def input_relay():
        for s in range(2):
            corner_copy(s).wait_recv()
            own = ig_part[(far_peer, side_peer)[s], half_rows(s), :].astype(jnp.float32)
            ig_mid[s] = (own + ig_in[s].astype(jnp.float32)).astype(jnp.bfloat16)
            relay_copy(s).start()

    def turn_cots(p):
        for kind in (GATE, UP):
            cots_turned[2 * p + kind] = cots[3 * p + kind].T

    def input_value(peer, some_parts):
        value = None
        for p in some_parts:
            for kind in (GATE, UP):
                block = jnp.concatenate(
                    [w_all[3 * p + kind, peer * pieces + i] for i in range(pieces)], axis=1
                )
                part = jnp.dot(
                    cots_turned[2 * p + kind], block, preferred_element_type=jnp.float32
                )
                value = part if value is None else value + part
        return value

    def input_base(turn):
        def body(peer, carry):
            ig_acc[peer] = input_value(peer, range(parts - 1))
            return carry

        share = n_tp // 2
        lax.fori_loop(turn * share, (turn + 1) * share, body, 0)

    def input_last():
        def body(step, carry):
            peer = jnp.where(
                step == 0, corner, jnp.where(step == 1, side_peer, jnp.where(step == 2, far_peer, tp))
            )
            value = ig_acc[peer] + input_value(peer, (parts - 1,))
            ig_part[peer] = value.astype(jnp.bfloat16)

            @pl.when(step == 0)
            def _():
                corner_copy(0).start()
                corner_copy(1).start()

            @pl.when(step == 1)
            def _():
                direct_copy(0).start()

            @pl.when(step == 2)
            def _():
                direct_copy(1).start()

            return carry

        lax.fori_loop(0, n_tp, body, 0)

    def drain_early(g, carry):
        for q in range(nz):
            gather_copy(g, q, SIBLING).wait_send()
            sibling_copy(g, chip_at(q)).wait_send()
        return carry

    def end_drain(g, carry):
        gather_copy(g, 0, inward).wait_send()
        return drain_early(g, carry)

    def middle_drain(g, carry):
        for q in (1, 2, 3):
            gather_copy(g, q, outward).wait_send()
        for q in (0, 1):
            gather_copy(g, q, inward).wait_send()
        return drain_early(g, carry)

    def end_gather(t, kind):
        gather_wait(t, 1, c)
        gather_copy(t, 1, SIBLING).start()
        pair_product(t, kind, 0, True)
        gather_wait(t, 2, c)
        gather_copy(t, 2, SIBLING).start()
        pair_product(t, kind, 1, False)
        gather_wait(t, 3, c)
        gather_copy(t, 3, SIBLING).start()
        pair_product(t, kind, 2, False)
        pair_product(t, kind, 3, False)

    def end_terms(low, high):
        def terms(g, carry):
            sibling_terms(g, (3, 2, 1, 0))
            return carry

        def own(g, carry):
            own_terms(g, (3, 2, 1, 0))
            return carry

        lax.fori_loop(low, high, terms, 0)
        lax.fori_loop(low, high, own, 0)

    def end_far(low, high):
        for q in (3, 2):
            def far(g, carry):
                send_sum(g, q, inward, False)
                return carry

            lax.fori_loop(low, high, far, 0)

    def end_near(low, high):
        def near(g, carry):
            send_sum(g, 1, inward, False)
            own_sum[g] = pair_sum(g, z)
            return carry

        lax.fori_loop(low, high, near, 0)

    def end_part(p, carry):
        first = 3 * p
        down = first + DOWN
        is_last = (p == parts - 1).astype(jnp.int32)

        def gate_or_up(kind, carry):
            @pl.when(p == parts - 1)
            def _():
                input_base(kind)

            end_gather(first + kind, kind)
            return carry

        lax.fori_loop(GATE, DOWN, gate_or_up, 0)
        make_hidden(p)
        end_terms(down, down + 1)
        end_far(down, down + 1)
        end_near(down + is_last, down + 1)

        end_gather(down, DOWN)
        make_cots(p)

        @pl.when(p == parts - 1)
        def _():
            turn_cots(p)
            input_last()

        end_terms(first, down)
        end_far(first, down)
        end_near(first, down + is_last)

        @pl.when(p < parts - 1)
        def _():
            turn_cots(p)
        return carry

    def relay_in(t):
        @pl.when(t < total)
        def _():
            gather_wait(t, 0, c)
            gather_copy(t, 0, inward).start()
            gather_copy(t, 0, SIBLING).start()

        @pl.when(jnp.logical_and(t + OWN_IN >= FIRST_IN, t + OWN_IN < total))
        def _():
            gather_copy(t + OWN_IN, 1, inward).start()

    def relay_near(t):
        @pl.when(t < total)
        def _():
            gather_wait(t, 2, c)
            gather_copy(t, 2, outward).start()
            gather_copy(t, 2, SIBLING).start()

    def relay_far(t):
        @pl.when(t < total)
        def _():
            gather_wait(t, 3, c)
            gather_copy(t, 3, outward).start()
            gather_copy(t, 3, SIBLING).start()

        @pl.when(jnp.logical_and(t + OWN_OUT >= FIRST_OUT, t + OWN_OUT < total))
        def _():
            gather_copy(t + OWN_OUT, 1, outward).start()

    def middle_gather(t, kind):
        relay_in(t + RELAY_IN)
        pair_product(t, kind, 1, True)
        relay_near(t + RELAY_OUT)
        pair_product(t, kind, 0, False)
        relay_far(t + RELAY_OUT)
        pair_product(t, kind, 2, False)
        pair_product(t, kind, 3, False)

    def in_turn(i):
        return 3 * (i // 3) + lax.rem(i + 2, 3)

    def final(r, carry):
        g = in_turn(r)
        line_copy(g, outward, z).wait_recv()
        own_sum[g] += line_in[g, outward, z].astype(jnp.float32)
        return carry

    def middle_final(r, carry):
        g = in_turn(r)
        for way in (inward, outward):
            line_copy(g, way, z).wait_recv()
        own_sum[g] += (
            line_in[g, inward, z].astype(jnp.float32) + line_in[g, outward, z].astype(jnp.float32)
        )
        return carry

    def middle_reduce(r):
        @pl.when(jnp.logical_and(r >= -1, r < total - 1))
        def _():
            g = in_turn(r + 1)
            sibling_terms(g, (3, 2, 0, 1))
            own_terms(g, (3, 2, 0, 1))

        @pl.when(jnp.logical_and(r >= 0, r < total))
        def _():
            send_sum(in_turn(r), 3, inward, True)

        @pl.when(jnp.logical_and(r >= LAG_OUT, r < total + LAG_OUT))
        def _():
            send_sum(in_turn(r - LAG_OUT), 0, outward, True)

        @pl.when(jnp.logical_and(r >= LAG_NEAR, r < total + LAG_NEAR))
        def _():
            g = in_turn(r - LAG_NEAR)
            send_sum(g, 2, inward, True)
            own_sum[g] = pair_sum(g, z)

        @pl.when(r >= LAG_FINAL)
        def _():
            middle_final(r - LAG_FINAL, 0)

    def middle_part(p, carry):
        for kind in (GATE, UP, DOWN):
            t = 3 * p + kind
            middle_gather(t, kind)
            if kind == UP:
                make_hidden(p)
            if kind == DOWN:
                make_cots(p)
            middle_reduce(t - LAG)
        turn_cots(p)
        return carry

    def middle_rest(r, carry):
        middle_reduce(r)
        turn = r - (total - LAG)

        @pl.when(turn < 2)
        def _():
            input_base(turn)

        @pl.when(turn == 2)
        def _():
            input_last()

        @pl.when(jnp.logical_and(turn > 2, turn < 8))
        def _():
            lax.fori_loop((turn - 3) * 2, (turn - 2) * 2, middle_drain, 0)

        @pl.when(turn == INPUT_TURN)
        def _():
            input_relay()

        return carry

    for t in range(total):
        if t == FIRST_OUT:
            for load in loads[total:]:
                load.start()
        loads[t].wait()
        gather_copy(t, jnp.where(is_end, 0, 1), SIBLING).start()

        @pl.when(is_end)
        def _():
            gather_copy(t, 0, inward).start()

        if t < FIRST_OUT:
            @pl.when(jnp.logical_not(is_end))
            def _():
                gather_copy(t, 1, outward).start()

        if t < FIRST_IN:
            @pl.when(jnp.logical_not(is_end))
            def _():
                gather_copy(t, 1, inward).start()

    for load in loads[total:]:
        load.wait()

    @pl.when(is_end)
    def _():
        lax.fori_loop(0, parts, end_part, 0)
        input_relay()
        lax.fori_loop(0, total, end_drain, 0)
        lax.fori_loop(0, total, final, 0)

    @pl.when(jnp.logical_not(is_end))
    def _():
        for t in range(RELAY_IN):
            relay_in(t)
        for t in range(RELAY_OUT):
            relay_near(t)
            relay_far(t)
        lax.fori_loop(0, parts, middle_part, 0)
        lax.fori_loop(total - LAG, total + LAG_OUT, middle_rest, 0)
        lax.fori_loop(total - 2, total, middle_drain, 0)
        lax.fori_loop(total + LAG_OUT - LAG_FINAL, total, middle_final, 0)

    for s in range(2):
        direct_copy(s).wait_recv()
        relay_copy(s).wait_recv()
        value = ig_part[tp, half_rows(s), :].astype(jnp.float32)
        for k in (2 + s, 4 + s):
            value = value + ig_in[k].astype(jnp.float32)
        ig_out[half_rows(s), :] = value.astype(ig_out.dtype)

    def drain_lines(r, carry):
        g = in_turn(r)
        for q in range(nz):
            chip = chip_at(q)

            @pl.when(chip != z)
            def _():
                way = jnp.where(chip > z, RIGHT, LEFT)
                line_copy(g, way, chip).wait_send()

        return carry

    lax.fori_loop(0, total, drain_lines, 0)
    for s in range(2):
        for copy in (corner_copy, direct_copy, relay_copy):
            copy(s).wait_send()


def fused_shards(tokens, cotangent, gate_weight, up_weight, down_weight):
    n, n_tp = lax.axis_size("fs"), lax.axis_size("tp")
    nz = n // 2
    count, width = tokens.shape
    rows, hidden = gate_weight.shape
    height = hidden // PARTS
    pieces = 3 * PARTS
    share = width // n_tp
    bf16, f32 = jnp.bfloat16, jnp.float32
    dma = pltpu.SemaphoreType.DMA
    input_grad, sums = pl.pallas_call(
        functools.partial(kernel, n, n_tp, PARTS),
        out_shape=(pltpu.VMEM((count, share), bf16), pltpu.VMEM((pieces, height, rows), f32)),
        in_specs=[pl.BlockSpec(memory_space=pl.ANY)] * 5,
        out_specs=(pl.BlockSpec(memory_space=pltpu.VMEM),) * 2,
        scratch_shapes=[
            pltpu.VMEM((2, count, width), bf16),
            pltpu.VMEM((pieces, n, height, rows), bf16),
            pltpu.VMEM((3, height, count), f32),
            pltpu.VMEM((pieces, height, count), bf16),
            pltpu.VMEM((2 * PARTS, count, height), bf16),
            pltpu.VMEM((pieces, nz, height, rows), f32),
            pltpu.VMEM((pieces, nz, height, rows), bf16),
            pltpu.VMEM((pieces, nz, height, rows), bf16),
            pltpu.VMEM((pieces, nz, height, rows), bf16),
            pltpu.VMEM((pieces, 2, nz, height, rows), bf16),
            pltpu.VMEM((n_tp, count, share), f32),
            pltpu.VMEM((n_tp, count, share), bf16),
            pltpu.VMEM((6, count // 2, share), bf16),
            pltpu.VMEM((2, count // 2, share), bf16),
            dma((pieces + 2,)),
            dma((pieces, 3, nz)),
            dma((pieces, n)),
            dma((pieces, nz)),
            dma((pieces, nz)),
            dma((pieces, nz)),
            dma((pieces, 2, nz)),
            dma((6,)),
            dma((6,)),
        ],
        compiler_params=pltpu.CompilerParams(
            collective_id=0, has_side_effects=True, vmem_limit_bytes=VMEM_BYTES
        ),
    )(tokens, cotangent, gate_weight.T, up_weight.T, down_weight.T)
    input_grad, gate_grad, up_grad, down_grad = pl.pallas_call(
        functools.partial(deliver, PARTS),
        out_shape=(
            jax.ShapeDtypeStruct((count, share), bf16),
        ) + (jax.ShapeDtypeStruct((hidden, rows), f32),) * 3,
        in_specs=[pl.BlockSpec(memory_space=pltpu.VMEM)] * 2,
        out_specs=(pl.BlockSpec(memory_space=pl.ANY),) * 4,
        scratch_shapes=[dma((pieces + 1,))],
        compiler_params=pltpu.CompilerParams(vmem_limit_bytes=DELIVER_BYTES),
    )(*(pltpu.with_memory_space_constraint(v, pltpu.VMEM) for v in (input_grad, sums)))
    return input_grad, gate_grad.T, up_grad.T, down_grad.T


def deliver(parts, ig, sums, ig_out, gate_out, up_out, down_out, sem):
    height = sums.shape[1]
    copies = [pltpu.make_async_copy(ig, ig_out, sem.at[3 * parts])]
    for g in range(3 * parts):
        out = (gate_out, up_out, down_out)[g % 3]
        piece = pl.ds((g // 3) * height, height)
        copies.append(pltpu.make_async_copy(sums.at[g], out.at[piece, :], sem.at[g]))
    for copy in copies:
        copy.start()
    for copy in copies:
        copy.wait()


def shards(tokens, cotangent, gate_weight, up_weight, down_weight):
    n, n_tp = lax.axis_size("fs"), lax.axis_size("tp")
    rows = gate_weight.shape[0]
    share = tokens.shape[1] // n_tp
    if n == 2 * CHIPS and n_tp == 4 and rows % 128 == 0 and share % rows == 0 and (
        gate_weight.shape[1] % (16 * PARTS) == 0
    ):
        return fused_shards(tokens, cotangent, gate_weight, up_weight, down_weight)
    return plain_shards(tokens, cotangent, gate_weight, up_weight, down_weight)


def solution(mesh):
    in_specs = (P("fs", None), P("fs", None), P("fs", "tp"), P("fs", "tp"), P("fs", "tp"))
    out_specs = (P("fs", "tp"), P("fs", "tp"), P("fs", "tp"), P("fs", "tp"))
    return jax.shard_map(shards, mesh=mesh, in_specs=in_specs, out_specs=out_specs, check_vma=False)
```
